1024 devices in a mesh: sp: 128 (over z, y), tp: 8 (over x, core).
Axes of the slice: x: 4, y: 8, z: 16, core: 2. Of those that a mesh axis runs over, the one named last changes fastest.
Arguments:
- tokens: bfloat16 [4, 16384, 2048], P(None, 'sp'), may hold values from -6 to 6
- next_tokens: bfloat16 [4, 2048], replicated, may hold values from -6 to 6
- w_query: bfloat16 [2048, 2048], P(None, 'tp'), may hold values from -0.125 to 0.125
- w_key: bfloat16 [2048, 2048], P(None, 'tp'), may hold values from -0.125 to 0.125
- w_value: bfloat16 [2048, 2048], P(None, 'tp'), may hold values from -0.125 to 0.125
- w_in_gate: bfloat16 [2048, 8], replicated, may hold values from -0.125 to 0.125
- w_forget_gate: bfloat16 [2048, 8], replicated, may hold values from -0.125 to 0.125
- forget_bias: float32 [8], replicated, may hold values from 3 to 14
- extra_decay: float32 [8, 4, 16384], P('tp', None, 'sp'), may hold values from -0.55006104 to 0
- w_out: bfloat16 [2048, 2048], P('tp'), may hold values from -0.125 to 0.125
Outputs:
- memory: bfloat16 [8, 1024, 256], P('tp', 'sp')
- normalizer: float32 [8, 1024], P('tp', 'sp')
- stabilizer: float32 [4, 8], P(None, 'tp')
- read: bfloat16 [4, 2048], replicated
The draws below stay inside these ranges and needn't reach their ends.
All inputs are finite; a program needn't handle non-finite values.
Results may differ from the reference program's by a relative error of at most 0.024.
Values may be sent and summed in bfloat16 or wider, within the bound.
No kernel may reach another device: no remote copies, remote signals or barrier semaphores. Data moves between devices by JAX's collectives and lax.ppermute only.
A program may use at most 32 MiB of HBM per device.

```python
import jax
import jax.numpy as jnp
from jax import lax

D = 2048
H = 8
HD = 256
SEQS = 4
TOK_DEV = 512
LENGTH = 16384
N_TP = 8


def draw_forget_bias(key, part):
    first, second, third = jax.random.split(key, 3)
    order = jax.random.permutation(first, H)
    slow = order < H // 2
    high = jax.random.uniform(second, (H,), jnp.float32, minval=11.0, maxval=14.0)
    low = jax.random.uniform(third, (H,), jnp.float32, minval=3.0, maxval=5.0)
    return jnp.where(slow, high, low)


def draw_extra_decay(key, part):
    first, second, third = jax.random.split(key, 3)
    span = TOK_DEV // SEQS
    blocks = LENGTH // span
    rate = jnp.exp(jax.random.uniform(first, (H, SEQS, blocks), jnp.float32, minval=jnp.log(0.2), maxval=0.0)) / LENGTH
    base = -jnp.repeat(rate, span, axis=2)
    hits = jax.random.randint(second, (H, SEQS, LENGTH), 0, LENGTH) < 3
    drop = jax.random.uniform(third, (H, SEQS, LENGTH), jnp.float32, minval=0.22, maxval=0.5)
    return base - jnp.where(hits, drop, 0.0)


def steps_of(rng, shape, shards, low, largest):
    loudness, own = 1.0, jax.random.fold_in(rng, 6)
    for dim, parts in shards:
        steps = jnp.exp(jax.random.uniform(jax.random.fold_in(own, dim), (parts,), jnp.float32, low / len(shards), largest / len(shards)))
        loudness = loudness * jnp.repeat(steps, shape[dim] // parts).reshape([-1 if axis == dim else 1 for axis in range(len(shape))])
    return loudness


def normal_values(stream_key, extent, deviation, most, shards=(), held_as=jnp.bfloat16):
    result = jax.random.normal(stream_key, extent, jnp.float32) * deviation
    if len(shards) > 0:
        result = steps_of(stream_key, extent, shards, -0.22, 0.18) * result
    return jnp.clip(result, min=-most, max=most).astype(held_as)


def setup_inputs(seed: int = 0) -> dict:
    key_list = jax.random.split(jax.random.key(seed), 11)
    return {
        "tokens": normal_values(key_list[0], (SEQS, LENGTH, D), 1.0, 6.0, ((1, 128),)),
        "next_tokens": normal_values(key_list[1], (SEQS, D), 1.0, 6.0),
        "w_query": normal_values(key_list[2], (D, H * HD), D ** -0.5, 0.125, ((1, 8),)),
        "w_key": normal_values(key_list[3], (D, H * HD), D ** -0.5, 0.125, ((1, 8),)),
        "w_value": normal_values(key_list[4], (D, H * HD), D ** -0.5, 0.125, ((1, 8),)),
        "w_in_gate": normal_values(key_list[5], (D, H), D ** -0.5, 0.125),
        "w_forget_gate": normal_values(key_list[6], (D, H), D ** -0.5, 0.125),
        "forget_bias": draw_forget_bias(jax.random.fold_in(key_list[10], 71), 0),
        "extra_decay": draw_extra_decay(jax.random.fold_in(key_list[10], 71), 0),
        "w_out": normal_values(key_list[9], (H * HD, D), (H * HD) ** -0.5, 0.125, ((0, 8),)),
    }


def reference(tokens, next_tokens, w_query, w_key, w_value, w_in_gate, w_forget_gate, forget_bias, extra_decay, w_out):
    scale = HD ** -0.5
    flat = tokens.reshape(SEQS * LENGTH, D)
    keys = jnp.dot(flat, w_key, preferred_element_type=jnp.float32).astype(jnp.bfloat16)
    values = jnp.dot(flat, w_value, preferred_element_type=jnp.float32).astype(jnp.bfloat16)
    log_in = jnp.dot(flat, w_in_gate, preferred_element_type=jnp.float32).reshape(SEQS, LENGTH, H)
    log_forget = jax.nn.log_sigmoid(jnp.dot(flat, w_forget_gate, preferred_element_type=jnp.float32) + forget_bias).reshape(SEQS, LENGTH, H) + jnp.transpose(extra_decay, (1, 2, 0))
    prefix = jnp.cumsum(log_forget, axis=1)
    total = prefix[:, -1]
    score = total[:, None, :] - prefix + log_in
    stabilizer = jnp.maximum(total, jnp.max(score, axis=1))
    weight = jnp.exp(score - stabilizer[:, None, :]) * scale
    keys4 = keys.reshape(SEQS, LENGTH, H, HD)
    values4 = values.reshape(SEQS, LENGTH, H, HD)

    def one_prompt(items):
        key_rows, value_rows, weight_rows = items
        weighted = (key_rows.astype(jnp.float32) * weight_rows[:, :, None]).astype(jnp.bfloat16)
        state = jnp.einsum('lhd,lhe->hde', weighted.astype(jnp.float32), value_rows.astype(jnp.float32))
        norm_state = jnp.sum(weighted.astype(jnp.float32), axis=0)
        return state, norm_state

    state, norm_state = lax.map(one_prompt, (keys4, values4, weight))
    memory = jnp.transpose(state, (1, 0, 2, 3)).reshape(H, SEQS * HD, HD).astype(jnp.bfloat16)
    normalizer = jnp.transpose(norm_state, (1, 0, 2)).reshape(H, SEQS * HD)
    query = jnp.dot(next_tokens, w_query, preferred_element_type=jnp.float32).astype(jnp.bfloat16).astype(jnp.float32).reshape(SEQS, H, HD)
    new_key = jnp.dot(next_tokens, w_key, preferred_element_type=jnp.float32).astype(jnp.bfloat16).astype(jnp.float32).reshape(SEQS, H, HD) * scale
    new_value = jnp.dot(next_tokens, w_value, preferred_element_type=jnp.float32).astype(jnp.bfloat16).astype(jnp.float32).reshape(SEQS, H, HD)
    new_in = jnp.dot(next_tokens, w_in_gate, preferred_element_type=jnp.float32)
    new_forget = jax.nn.log_sigmoid(jnp.dot(next_tokens, w_forget_gate, preferred_element_type=jnp.float32) + forget_bias)
    query_state = jnp.einsum('shd,shde->she', query, state, precision=lax.Precision.HIGHEST)
    query_norm = jnp.sum(query * norm_state, axis=-1)
    top = jnp.maximum(new_forget + stabilizer, new_in)
    keep = jnp.exp(new_forget + stabilizer - top)
    take = jnp.exp(new_in - top)
    qk = jnp.sum(query * new_key, axis=-1)
    numer = keep[:, :, None] * query_state + (take * qk)[:, :, None] * new_value
    denom = keep * query_norm + take * qk
    head_out = (numer / jnp.maximum(jnp.abs(denom), 1.0)[:, :, None]).astype(jnp.bfloat16)
    grouped = head_out.reshape(SEQS, N_TP, (H // N_TP) * HD).astype(jnp.float32)
    out_rows = w_out.reshape(N_TP, (H // N_TP) * HD, D).astype(jnp.float32)
    partial_sums = jnp.einsum('sgc,gcd->gsd', grouped, out_rows).astype(jnp.bfloat16)
    read = jnp.sum(partial_sums.astype(jnp.float32), axis=0).astype(jnp.bfloat16)
    return memory, normalizer, stabilizer, read
```

```python
import functools

import jax
import jax.numpy as jnp
from jax import lax
from jax.experimental import pallas as pl
from jax.experimental.pallas import tpu as pltpu
from jax.sharding import Mesh
from jax.sharding import PartitionSpec as P

HD = 256
SP = ("sp_0", "sp_1")
LANES = 128
F32 = jnp.float32
BF16 = jnp.bfloat16

NT = (((1,), (1,)), ((), ()))
TN = (((0,), (0,)), ((), ()))


def parts3(x):
    hi = x.astype(BF16).astype(F32)
    rest = x - hi
    mid = rest.astype(BF16).astype(F32)
    return hi, mid, rest - mid


def log_sigmoid(x):
    return jnp.minimum(x, 0.0) - jnp.log1p(jnp.exp(-jnp.abs(x)))


def lanes_of(shape):
    return lax.broadcasted_iota(jnp.int32, shape, len(shape) - 1)


def row_of_head(w_ref, head):
    rows = lax.broadcasted_iota(jnp.int32, w_ref.shape, 0)
    picked = jnp.where(rows == head, w_ref[...].astype(F32), 0.0)
    return jnp.sum(picked, axis=0, keepdims=True)


def stat_rows(total, query_norm, peak):
    at = lanes_of(total.shape)
    packed = jnp.where(at < 4, total, jnp.where(at < 8, query_norm, peak))
    return jnp.concatenate(parts3(packed), axis=0)


def stats_from(rows):
    total = rows
    query_norm = pltpu.roll(rows, LANES - 4, 1)
    peak = pltpu.roll(rows, LANES - 8, 1)
    return total, query_norm, peak


def later_sums(total):
    later = [jnp.zeros_like(total[:1])]
    for i in range(total.shape[0] - 1, 0, -1):
        later.append(later[-1] + total[i : i + 1])
    later.reverse()
    return later


def block_kernel(
    seqs,
    n_y,
    tokens_ref,
    next_ref,
    w_query_ref,
    w_key_ref,
    w_value_ref,
    in_gate_ref,
    forget_gate_ref,
    bias_ref,
    decay_ref,
    out_ref,
):
    head = lax.axis_index("tp")
    span = tokens_ref.shape[0] // seqs
    scale = HD ** (-0.5)
    tokens = tokens_ref[...]
    keys = jnp.dot(tokens, w_key_ref[...], preferred_element_type=F32).astype(BF16)
    values = jnp.dot(tokens, w_value_ref[...], preferred_element_type=F32).astype(BF16)
    depth = tokens.shape[1]
    gate_rows = jnp.concatenate(
        [
            jnp.broadcast_to(row_of_head(in_gate_ref, head), (LANES, depth)),
            jnp.broadcast_to(row_of_head(forget_gate_ref, head), (LANES, depth)),
        ],
        axis=0,
    ).astype(BF16)
    gates = lax.dot_general(tokens, gate_rows, NT, preferred_element_type=F32)
    query = jnp.dot(next_ref[...], w_query_ref[...], preferred_element_type=F32).astype(BF16)

    prompt = lanes_of((span, LANES)) % seqs
    log_in = gates[:span, :LANES]
    forget = gates[:span, LANES:]
    for p in range(1, seqs):
        rows = slice(p * span, (p + 1) * span)
        log_in = jnp.where(prompt == p, gates[rows, :LANES], log_in)
        forget = jnp.where(prompt == p, gates[rows, LANES:], forget)
    decay = jnp.transpose(jnp.concatenate([decay_ref[...]] * (LANES // seqs), axis=0))
    log_forget = log_sigmoid(forget + bias_ref[head]) + decay
    after = (
        lax.broadcasted_iota(jnp.int32, (span, span), 1)
        > lax.broadcasted_iota(jnp.int32, (span, span), 0)
    ).astype(BF16)
    suffix = jnp.zeros((span, LANES), F32)
    for part in parts3(log_forget):
        suffix += jnp.dot(after, part.astype(BF16), preferred_element_type=F32)
    total = suffix[:1] + log_forget[:1]
    score = suffix + log_in
    peak = jnp.max(score, axis=0, keepdims=True)
    weight = jnp.exp(score - peak) * scale

    at = lanes_of((1, LANES)) % seqs
    query_norm = jnp.zeros((1, LANES), F32)
    ones = jnp.ones((8, span), BF16)
    high, low, norms = [], [], []
    run = HD // 4
    for p in range(seqs):
        rows = slice(p * span, (p + 1) * span)
        weighted = (keys[rows].astype(F32) * weight[:, p : p + 1]).astype(BF16)
        memory = lax.dot_general(weighted, values[rows], TN, preferred_element_type=F32)
        norms.append(jnp.dot(ones, weighted, preferred_element_type=F32)[:1])
        along = lax.dot_general(query, weighted, NT, preferred_element_type=F32)[p : p + 1]
        query_norm = jnp.where(at == p, jnp.sum(along, axis=1, keepdims=True), query_norm)
        stacked = jnp.concatenate(parts3(along) + (jnp.zeros((5, span), F32),), axis=0)
        reads = jnp.dot(stacked.astype(BF16), values[rows], preferred_element_type=F32)
        read = jnp.sum(reads, axis=0, keepdims=True)
        read_high = read.astype(BF16).astype(F32)
        high.append(read_high)
        low.append(read - read_high)
        for y in range(n_y):
            pieces = [memory[r * run + y * 8 : r * run + y * 8 + 8] for r in range(4)]
            out_ref[y, p * 32 : (p + 1) * 32, :] = jnp.concatenate(pieces, axis=0).astype(BF16)
    stats = stat_rows(total, query_norm, peak)
    wide = jnp.concatenate([stats, jnp.zeros_like(stats)], axis=1)
    extra = jnp.concatenate(high + low + norms + [wide, jnp.zeros((1, HD), F32)], axis=0)
    extra = extra.astype(BF16)
    for y in range(n_y):
        out_ref[y, 128:144, :] = extra


def group_kernel(seqs, n_y, n_z, in_ref, out_ref):
    extras = [in_ref[y, 128:144, :].astype(F32) for y in range(n_y)]
    rows = jnp.concatenate(
        [e[12:13, :LANES] + e[13:14, :LANES] + e[14:15, :LANES] for e in extras], axis=0
    )
    total, query_norm, peak = stats_from(rows)
    later = later_sums(total)
    scores = [later[y] + peak[y : y + 1] for y in range(n_y)]
    group_total = later[0] + total[:1]
    group_peak = functools.reduce(jnp.maximum, scores)
    coef = jnp.exp(jnp.concatenate(scores, axis=0) - group_peak)
    group_norm = jnp.sum(coef * query_norm, axis=0, keepdims=True)
    tall = jnp.transpose(jnp.concatenate([coef] * (LANES // n_y), axis=0))
    per_y = [jnp.broadcast_to(tall[:8, y : y + 1], (8, HD)) for y in range(n_y)]

    at = lanes_of((1, LANES))
    stats = stat_rows(
        group_total, pltpu.roll(jnp.broadcast_to(group_norm, (8, LANES)), 4, 1)[:1],
        pltpu.roll(jnp.broadcast_to(group_peak, (8, LANES)), 8, 1)[:1],
    )
    stats = jnp.where(at < 12, stats, 0.0)
    wide = jnp.concatenate([stats, jnp.zeros_like(stats)], axis=1)
    reads = jnp.zeros((seqs, HD), F32)
    norms = jnp.zeros((seqs, HD), F32)
    for y in range(n_y):
        c = per_y[y][:seqs]
        e = extras[y]
        reads += c * (e[:seqs] + e[seqs : 2 * seqs])
        norms += c * e[2 * seqs : 3 * seqs]
    for p in range(seqs):
        memory = jnp.zeros((32, HD), F32)
        for y in range(n_y):
            memory += per_y[y][p : p + 1] * in_ref[y, p * 32 : (p + 1) * 32, :].astype(F32)
        tail = jnp.concatenate([reads, wide, norms[p : p + 1]], axis=0)
        for r in range(n_z // seqs):
            block = jnp.concatenate([memory[r * 8 : r * 8 + 8], tail], axis=0)
            out_ref[p * (n_z // seqs) + r] = block.astype(BF16)


def final_kernel(
    seqs,
    n_z,
    n_tp,
    in_ref,
    query_ref,
    key_ref,
    value_ref,
    new_in_ref,
    new_forget_ref,
    w_out_ref,
    memory_ref,
    norm_ref,
    stab_ref,
    head_ref,
):
    z = lax.axis_index("sp_0")
    y = lax.axis_index("sp_1")
    per_prompt = n_z // seqs
    mine = z // per_prompt
    blocks = [in_ref[i].astype(F32) for i in range(n_z)]
    rows = jnp.concatenate(
        [b[12:13, :LANES] + b[13:14, :LANES] + b[14:15, :LANES] for b in blocks], axis=0
    )
    total, query_norm, peak = stats_from(rows)
    later = later_sums(total)
    scores = [later[i] + peak[i : i + 1] for i in range(n_z)]
    stab = functools.reduce(jnp.maximum, scores, later[0] + total[:1])
    coef = jnp.exp(jnp.concatenate(scores, axis=0) - stab)
    all_norm = jnp.sum(coef * query_norm, axis=0, keepdims=True)
    filled = jnp.zeros((LANES - n_z - 2, LANES), F32)
    tall = jnp.transpose(jnp.concatenate([coef, stab, all_norm, filled], axis=0))[:8]
    stab4 = tall[:seqs, n_z : n_z + 1]
    query_norm4 = tall[:seqs, n_z + 1 : n_z + 2]
    stab_ref[...] = stab4

    is_mine = lanes_of(coef.shape) == mine
    own = jnp.sum(jnp.where(is_mine, coef, 0.0), axis=1, keepdims=True)
    memory = jnp.zeros((8, HD), F32)
    norm = jnp.zeros((1, HD), F32)
    query_state = jnp.zeros((seqs, HD), F32)
    for i in range(n_z):
        memory += own[i : i + 1] * blocks[i][:8]
        norm += own[i : i + 1] * blocks[i][15:16]
        query_state += tall[:seqs, i : i + 1] * blocks[i][8:12]
    memory_ref[...] = memory.astype(BF16)
    first = lax.rem(z, per_prompt) * (HD // per_prompt) + y * 8
    turned = pltpu.roll(jnp.broadcast_to(norm, (8, HD)), lax.rem(HD - first, HD), 1)
    norm_ref[...] = turned[:1, :8]

    query = query_ref[...]
    new_key = key_ref[...]
    new_value = value_ref[...]
    new_in = new_in_ref[...]
    carried = new_forget_ref[...] + stab4
    top = jnp.maximum(carried, new_in)
    keep = jnp.exp(carried - top)
    take = jnp.exp(new_in - top)
    qk = jnp.sum(query * new_key, axis=1, keepdims=True)
    numer = keep * query_state + take * qk * new_value
    denom = keep * query_norm4 + take * qk
    head_out = (numer / jnp.maximum(jnp.abs(denom), 1.0)).astype(BF16)
    partial = jnp.dot(head_out, w_out_ref[...], preferred_element_type=F32).astype(BF16)
    for i in range(n_tp):
        head_ref[i] = partial


def per_device(
    tokens,
    next_tokens,
    w_query,
    w_key,
    w_value,
    w_in_gate,
    w_forget_gate,
    forget_bias,
    extra_decay,
    w_out,
):
    scale = HD ** (-0.5)
    seqs, span, depth = tokens.shape
    n_z, n_y, n_tp = (lax.axis_size(a) for a in ("sp_0", "sp_1", "tp"))
    whole = pl.BlockSpec(memory_space=pltpu.VMEM)
    scalar = pl.BlockSpec(memory_space=pltpu.SMEM)

    sent = pl.pallas_call(
        functools.partial(block_kernel, seqs, n_y),
        out_shape=jax.ShapeDtypeStruct((n_y, 144, HD), BF16),
        in_specs=[whole] * 7 + [scalar, whole],
        out_specs=whole,
        cost_estimate=pl.CostEstimate(
            flops=2 * seqs * span * depth * 3 * HD, bytes_accessed=6 << 20, transcendentals=0
        ),
    )(
        tokens.reshape(seqs * span, depth),
        next_tokens,
        w_query,
        w_key,
        w_value,
        w_in_gate.T,
        w_forget_gate.T,
        forget_bias,
        extra_decay.reshape(seqs, span),
    )
    arrived = lax.all_to_all(sent, "sp_1", 0, 0, tiled=True)

    head = lax.axis_index("tp")
    gate_in = lax.dynamic_slice_in_dim(w_in_gate, head, 1, 1)
    gate_forget = lax.dynamic_slice_in_dim(w_forget_gate, head, 1, 1)
    bias_here = lax.dynamic_slice_in_dim(forget_bias, head, 1, 0)

    def rounded(w):
        return jnp.dot(next_tokens, w, preferred_element_type=F32).astype(BF16).astype(F32)

    query = rounded(w_query)
    new_key = rounded(w_key) * scale
    new_value = rounded(w_value)
    new_in = jnp.dot(next_tokens, gate_in, preferred_element_type=F32)
    new_forget = jax.nn.log_sigmoid(
        jnp.dot(next_tokens, gate_forget, preferred_element_type=F32) + bias_here
    )

    group = pl.pallas_call(
        functools.partial(group_kernel, seqs, n_y, n_z),
        out_shape=jax.ShapeDtypeStruct((n_z, 16, HD), BF16),
        in_specs=[whole],
        out_specs=whole,
    )(arrived)
    gathered = lax.all_to_all(group, "sp_0", 0, 0, tiled=True)

    memory, norm, stab, partial = pl.pallas_call(
        functools.partial(final_kernel, seqs, n_z, n_tp),
        out_shape=(
            jax.ShapeDtypeStruct((8, HD), BF16),
            jax.ShapeDtypeStruct((1, 8), F32),
            jax.ShapeDtypeStruct((seqs, 1), F32),
            jax.ShapeDtypeStruct((n_tp, seqs, depth), BF16),
        ),
        in_specs=[whole] * 7,
        out_specs=(whole,) * 4,
    )(gathered, query, new_key, new_value, new_in, new_forget, w_out)
    parts = lax.all_to_all(partial, "tp", 0, 0, tiled=True)
    read = parts.astype(F32).sum(axis=0).astype(BF16)
    return memory[None], norm, stab, read


def solution(mesh):
    torus = Mesh(mesh.devices.reshape(16, 8, mesh.shape["tp"]), ("sp_0", "sp_1", "tp"))
    placed = (
        P(None, SP, None),
        P(),
        P(None, "tp"),
        P(None, "tp"),
        P(None, "tp"),
        P(),
        P(),
        P(),
        P("tp", None, SP),
        P("tp", None),
    )
    return jax.shard_map(
        per_device,
        mesh=torus,
        in_specs=placed,
        out_specs=(P("tp", SP, None), P("tp", SP), P(None, "tp"), P()),
        check_vma=False,
    )
```

```python
import functools

import jax
import jax.numpy as jnp
from jax import lax
from jax.experimental import pallas as pl
from jax.experimental.pallas import tpu as pltpu
from jax.sharding import Mesh
from jax.sharding import PartitionSpec as P

HD = 256
SP = ("sp_0", "sp_1")
LANES = 128
F32 = jnp.float32
BF16 = jnp.bfloat16

NT = (((1,), (1,)), ((), ()))
TN = (((0,), (0,)), ((), ()))


def parts3(x):
    hi = x.astype(BF16).astype(F32)
    rest = x - hi
    mid = rest.astype(BF16).astype(F32)
    return hi, mid, rest - mid


def log_sigmoid(x):
    return jnp.minimum(x, 0.0) - jnp.log1p(jnp.exp(-jnp.abs(x)))


def lanes_of(shape):
    return lax.broadcasted_iota(jnp.int32, shape, len(shape) - 1)


def stats_from(rows):
    return rows, pltpu.roll(rows, LANES - 4, 1), pltpu.roll(rows, LANES - 8, 1)


def later_sums(total):
    later = [jnp.zeros_like(total[:1])]
    for i in range(total.shape[0] - 1, 0, -1):
        later.append(later[-1] + total[i : i + 1])
    later.reverse()
    return later


def block_kernel(
    seqs,
    n_y,
    tokens_hbm,
    next_hbm,
    w_query_hbm,
    w_key_hbm,
    w_value_hbm,
    in_gate_hbm,
    forget_gate_hbm,
    bias_hbm,
    decay_hbm,
    out_hbm,
    tokens_ref,
    next_ref,
    w_query_ref,
    w_key_ref,
    w_value_ref,
    gate_ref,
    bias_ref,
    decay_ref,
    out_ref,
    sems,
    out_sems,
):
    head = lax.axis_index("tp")
    depth = tokens_ref.shape[1]
    heads = in_gate_hbm.shape[0]
    span = tokens_ref.shape[0] // seqs
    scale = HD ** (-0.5)
    moves = [
        (in_gate_hbm, gate_ref.at[pl.ds(0, heads)]),
        (forget_gate_hbm, gate_ref.at[pl.ds(heads, heads)]),
        (tokens_hbm, tokens_ref),
        (bias_hbm, bias_ref),
        (decay_hbm, decay_ref),
        (w_key_hbm, w_key_ref),
        (next_hbm, next_ref),
        (w_query_hbm, w_query_ref),
        (w_value_hbm, w_value_ref),
    ]
    copies = [pltpu.make_async_copy(a, b, sems.at[i]) for i, (a, b) in enumerate(moves)]
    for copy in copies:
        copy.start()
    after = (
        lax.broadcasted_iota(jnp.int32, (span, span), 0)
        > lax.broadcasted_iota(jnp.int32, (span, span), 1)
    ).astype(BF16)

    for copy in copies:
        copy.wait()
    gates = lax.dot_general(gate_ref[...], tokens_ref[...], NT, preferred_element_type=F32)
    row = lax.broadcasted_iota(jnp.int32, gates.shape, 0)
    log_in = jnp.sum(jnp.where(row == head, gates, 0.0), axis=0, keepdims=True)
    forget = jnp.sum(jnp.where(row == head + heads, gates, 0.0), axis=0, keepdims=True)
    log_in, forget = (
        jnp.concatenate([v[:, p * span : (p + 1) * span] for p in range(seqs)], axis=0)
        for v in (log_in, forget)
    )
    log_forget = log_sigmoid(forget + bias_ref[head]) + decay_ref[...]
    split = jnp.concatenate(parts3(log_forget) + (jnp.zeros((seqs, span), F32),), axis=0)
    sums = jnp.dot(split.astype(BF16), after, preferred_element_type=F32)
    suffix = sums[:seqs] + sums[seqs : 2 * seqs] + sums[2 * seqs : 3 * seqs]
    total = jnp.sum(log_forget, axis=1, keepdims=True)
    score = suffix + log_in
    peak = jnp.max(score, axis=1, keepdims=True)
    weight = jnp.exp(score - peak) * scale
    stats = [jnp.broadcast_to(v, (seqs, span)) for v in (total, peak)]
    fill = jnp.zeros((LANES - 3 * seqs, span), F32)
    turned = jnp.transpose(jnp.concatenate([weight] + stats + [fill], axis=0))

    keys = jnp.dot(tokens_ref[...], w_key_ref[...], preferred_element_type=F32)
    weighted = []
    for p in range(seqs):
        rows = slice(p * span, (p + 1) * span)
        rounded = keys[rows].astype(BF16).astype(F32)
        weighted.append((rounded * turned[:, p : p + 1]).astype(BF16))

    query = jnp.dot(next_ref[...], w_query_ref[...], preferred_element_type=F32).astype(BF16)
    values = jnp.dot(tokens_ref[...], w_value_ref[...], preferred_element_type=F32).astype(BF16)
    at = lanes_of((1, LANES))
    stats = jnp.where(at < seqs, 0.0, turned[:1])
    ones = jnp.ones((8, span), BF16)
    high, low, norms, sends = [], [], [], []
    run = HD // 4
    for p in range(seqs):
        rows = slice(p * span, (p + 1) * span)
        memory = lax.dot_general(weighted[p], values[rows], TN, preferred_element_type=F32)
        for y in range(n_y):
            pieces = [memory[r * run + y * 8 : r * run + y * 8 + 8] for r in range(4)]
            out_ref[y, p * 32 : (p + 1) * 32, :] = jnp.concatenate(pieces, axis=0).astype(BF16)
        part = pl.ds(p * 32, 32)
        sends.append(
            pltpu.make_async_copy(out_ref.at[:, part, :], out_hbm.at[:, part, :], out_sems.at[p])
        )
        sends[-1].start()
        norms.append(jnp.dot(ones, weighted[p], preferred_element_type=F32)[:1])
        along = lax.dot_general(query, weighted[p], NT, preferred_element_type=F32)[p : p + 1]
        stats = jnp.where(at == p, jnp.sum(along, axis=1, keepdims=True), stats)
        stacked = jnp.concatenate(parts3(along) + (jnp.zeros((5, span), F32),), axis=0)
        reads = jnp.dot(stacked.astype(BF16), values[rows], preferred_element_type=F32)
        read = jnp.sum(reads, axis=0, keepdims=True)
        read_high = read.astype(BF16).astype(F32)
        high.append(read_high)
        low.append(read - read_high)
    stats = jnp.concatenate(parts3(stats), axis=0)
    wide = jnp.concatenate([stats, jnp.zeros_like(stats)], axis=1)
    extra = jnp.concatenate(high + low + norms + [wide, jnp.zeros((1, HD), F32)], axis=0)
    extra = extra.astype(BF16)
    for y in range(n_y):
        out_ref[y, 128:144, :] = extra
    part = pl.ds(128, 16)
    sends.append(
        pltpu.make_async_copy(out_ref.at[:, part, :], out_hbm.at[:, part, :], out_sems.at[seqs])
    )
    sends[-1].start()
    for copy in sends:
        copy.wait()


def group_kernel(seqs, n_y, n_z, in_ref, out_ref):
    extras = [in_ref[y, 128:144, :].astype(F32) for y in range(n_y)]
    rows = jnp.concatenate(
        [e[12:13, :LANES] + e[13:14, :LANES] + e[14:15, :LANES] for e in extras], axis=0
    )
    query_norm, total, peak = stats_from(rows)
    later = later_sums(total)
    scores = [later[y] + peak[y : y + 1] for y in range(n_y)]
    group_total = later[0] + total[:1]
    group_peak = functools.reduce(jnp.maximum, scores)
    coef = jnp.exp(jnp.concatenate(scores, axis=0) - group_peak)
    group_norm = jnp.sum(coef * query_norm, axis=0, keepdims=True)
    tall = jnp.transpose(jnp.concatenate([coef] * (LANES // n_y), axis=0))
    per_y = [jnp.broadcast_to(tall[:8, y : y + 1], (8, HD)) for y in range(n_y)]

    at = lanes_of((1, LANES))
    total_there = pltpu.roll(jnp.broadcast_to(group_total, (8, LANES)), 4, 1)[:1]
    peak_there = pltpu.roll(jnp.broadcast_to(group_peak, (8, LANES)), 8, 1)[:1]
    packed = jnp.where(at < 4, group_norm, jnp.where(at < 8, total_there, peak_there))
    stats = jnp.concatenate(parts3(jnp.where(at < 12, packed, 0.0)), axis=0)
    wide = jnp.concatenate([stats, jnp.zeros_like(stats)], axis=1)
    reads = jnp.zeros((seqs, HD), F32)
    norms = jnp.zeros((seqs, HD), F32)
    for y in range(n_y):
        c = per_y[y][:seqs]
        e = extras[y]
        reads += c * (e[:seqs] + e[seqs : 2 * seqs])
        norms += c * e[2 * seqs : 3 * seqs]
    for p in range(seqs):
        memory = jnp.zeros((32, HD), F32)
        for y in range(n_y):
            memory += per_y[y][p : p + 1] * in_ref[y, p * 32 : (p + 1) * 32, :].astype(F32)
        tail = jnp.concatenate([reads, wide, norms[p : p + 1]], axis=0)
        for r in range(n_z // seqs):
            block = jnp.concatenate([memory[r * 8 : r * 8 + 8], tail], axis=0)
            out_ref[p * (n_z // seqs) + r] = block.astype(BF16)


def final_kernel(
    seqs,
    n_z,
    n_tp,
    in_ref,
    query_ref,
    key_ref,
    value_ref,
    new_in_ref,
    new_forget_ref,
    w_out_ref,
    memory_ref,
    norm_ref,
    stab_ref,
    head_ref,
):
    z = lax.axis_index("sp_0")
    y = lax.axis_index("sp_1")
    per_prompt = n_z // seqs
    mine = z // per_prompt
    blocks = [in_ref[i].astype(F32) for i in range(n_z)]
    rows = jnp.concatenate(
        [b[12:13, :LANES] + b[13:14, :LANES] + b[14:15, :LANES] for b in blocks], axis=0
    )
    query_norm, total, peak = stats_from(rows)
    later = later_sums(total)
    scores = [later[i] + peak[i : i + 1] for i in range(n_z)]
    stab = functools.reduce(jnp.maximum, scores, later[0] + total[:1])
    coef = jnp.exp(jnp.concatenate(scores, axis=0) - stab)
    all_norm = jnp.sum(coef * query_norm, axis=0, keepdims=True)
    filled = jnp.zeros((LANES - n_z - 2, LANES), F32)
    tall = jnp.transpose(jnp.concatenate([coef, stab, all_norm, filled], axis=0))[:8]
    stab4 = tall[:seqs, n_z : n_z + 1]
    query_norm4 = tall[:seqs, n_z + 1 : n_z + 2]
    stab_ref[...] = stab4

    is_mine = lanes_of(coef.shape) == mine
    own = jnp.sum(jnp.where(is_mine, coef, 0.0), axis=1, keepdims=True)
    memory = jnp.zeros((8, HD), F32)
    norm = jnp.zeros((1, HD), F32)
    query_state = jnp.zeros((seqs, HD), F32)
    for i in range(n_z):
        memory += own[i : i + 1] * blocks[i][:8]
        norm += own[i : i + 1] * blocks[i][15:16]
        query_state += tall[:seqs, i : i + 1] * blocks[i][8:12]
    memory_ref[...] = memory.astype(BF16)
    first = lax.rem(z, per_prompt) * (HD // per_prompt) + y * 8
    turned = pltpu.roll(jnp.broadcast_to(norm, (8, HD)), lax.rem(HD - first, HD), 1)
    norm_ref[...] = turned[:1, :8]

    query = query_ref[...]
    new_key = key_ref[...]
    new_value = value_ref[...]
    new_in = new_in_ref[...]
    carried = new_forget_ref[...] + stab4
    top = jnp.maximum(carried, new_in)
    keep = jnp.exp(carried - top)
    take = jnp.exp(new_in - top)
    qk = jnp.sum(query * new_key, axis=1, keepdims=True)
    numer = keep * query_state + take * qk * new_value
    denom = keep * query_norm4 + take * qk
    head_out = (numer / jnp.maximum(jnp.abs(denom), 1.0)).astype(BF16)
    partial = jnp.dot(head_out, w_out_ref[...], preferred_element_type=F32).astype(BF16)
    for i in range(n_tp):
        head_ref[i] = partial


def per_device(
    tokens,
    next_tokens,
    w_query,
    w_key,
    w_value,
    w_in_gate,
    w_forget_gate,
    forget_bias,
    extra_decay,
    w_out,
):
    scale = HD ** (-0.5)
    seqs, span, depth = tokens.shape
    n_z, n_y, n_tp = (lax.axis_size(a) for a in ("sp_0", "sp_1", "tp"))
    whole = pl.BlockSpec(memory_space=pltpu.VMEM)
    heads = w_in_gate.shape[1]
    hbm = pl.BlockSpec(memory_space=pl.ANY)

    sent = pl.pallas_call(
        functools.partial(block_kernel, seqs, n_y),
        out_shape=jax.ShapeDtypeStruct((n_y, 144, HD), BF16),
        in_specs=[hbm] * 9,
        out_specs=hbm,
        scratch_shapes=[
            pltpu.VMEM((seqs * span, depth), BF16),
            pltpu.VMEM((seqs, depth), BF16),
            pltpu.VMEM((depth, HD), BF16),
            pltpu.VMEM((depth, HD), BF16),
            pltpu.VMEM((depth, HD), BF16),
            pltpu.VMEM((2 * heads, depth), BF16),
            pltpu.SMEM((heads,), F32),
            pltpu.VMEM((seqs, span), F32),
            pltpu.VMEM((n_y, 144, HD), BF16),
            pltpu.SemaphoreType.DMA((9,)),
            pltpu.SemaphoreType.DMA((seqs + 1,)),
        ],
        cost_estimate=pl.CostEstimate(
            flops=2 * seqs * span * depth * 3 * HD, bytes_accessed=6 << 20, transcendentals=0
        ),
    )(
        tokens.reshape(seqs * span, depth),
        next_tokens,
        w_query,
        w_key,
        w_value,
        w_in_gate.T,
        w_forget_gate.T,
        forget_bias,
        extra_decay.reshape(seqs, span),
    )
    arrived = lax.all_to_all(sent, "sp_1", 0, 0, tiled=True)

    head = lax.axis_index("tp")
    gate_in = lax.dynamic_slice_in_dim(w_in_gate, head, 1, 1)
    gate_forget = lax.dynamic_slice_in_dim(w_forget_gate, head, 1, 1)
    bias_here = lax.dynamic_slice_in_dim(forget_bias, head, 1, 0)

    def rounded(w):
        return jnp.dot(next_tokens, w, preferred_element_type=F32).astype(BF16).astype(F32)

    query = rounded(w_query)
    new_key = rounded(w_key) * scale
    new_value = rounded(w_value)
    new_in = jnp.dot(next_tokens, gate_in, preferred_element_type=F32)
    new_forget = jax.nn.log_sigmoid(
        jnp.dot(next_tokens, gate_forget, preferred_element_type=F32) + bias_here
    )

    group = pl.pallas_call(
        functools.partial(group_kernel, seqs, n_y, n_z),
        out_shape=jax.ShapeDtypeStruct((n_z, 16, HD), BF16),
        in_specs=[whole],
        out_specs=whole,
        compiler_params=pltpu.CompilerParams(vmem_limit_bytes=16 << 20),
    )(arrived)
    gathered = lax.all_to_all(group, "sp_0", 0, 0, tiled=True)

    memory, norm, stab, partial = pl.pallas_call(
        functools.partial(final_kernel, seqs, n_z, n_tp),
        out_shape=(
            jax.ShapeDtypeStruct((8, HD), BF16),
            jax.ShapeDtypeStruct((1, 8), F32),
            jax.ShapeDtypeStruct((seqs, 1), F32),
            jax.ShapeDtypeStruct((n_tp, seqs, depth), BF16),
        ),
        in_specs=[whole] * 7,
        out_specs=(whole,) * 4,
        compiler_params=pltpu.CompilerParams(vmem_limit_bytes=16 << 20),
    )(gathered, query, new_key, new_value, new_in, new_forget, w_out)
    parts = lax.all_to_all(partial, "tp", 0, 0, tiled=True)
    read = parts.astype(F32).sum(axis=0).astype(BF16)
    return memory[None], norm, stab, read


def solution(mesh):
    torus = Mesh(mesh.devices.reshape(16, 8, mesh.shape["tp"]), ("sp_0", "sp_1", "tp"))
    placed = (
        P(None, SP, None),
        P(),
        P(None, "tp"),
        P(None, "tp"),
        P(None, "tp"),
        P(),
        P(),
        P(),
        P("tp", None, SP),
        P("tp", None),
    )
    return jax.shard_map(
        per_device,
        mesh=torus,
        in_specs=placed,
        out_specs=(P("tp", SP, None), P("tp", SP), P(None, "tp"), P()),
        check_vma=False,
    )
```

```python
import functools

import jax
import jax.numpy as jnp
from jax import lax
from jax.experimental import pallas as pl
from jax.experimental.pallas import tpu as pltpu
from jax.sharding import Mesh
from jax.sharding import PartitionSpec as P

HD = 256
SP = ("sp_0", "sp_1")
LANES = 128
F32 = jnp.float32
BF16 = jnp.bfloat16

NT = (((1,), (1,)), ((), ()))
TN = (((0,), (0,)), ((), ()))


def parts3(x):
    hi = x.astype(BF16).astype(F32)
    rest = x - hi
    mid = rest.astype(BF16).astype(F32)
    return hi, mid, rest - mid


def log_sigmoid(x):
    return jnp.minimum(x, 0.0) - jnp.log1p(jnp.exp(-jnp.abs(x)))


def lanes_of(shape):
    return lax.broadcasted_iota(jnp.int32, shape, len(shape) - 1)


def stats_from(rows):
    return rows, pltpu.roll(rows, LANES - 4, 1), pltpu.roll(rows, LANES - 8, 1)


def later_sums(total):
    later = [jnp.zeros_like(total[:1])]
    for i in range(total.shape[0] - 1, 0, -1):
        later.append(later[-1] + total[i : i + 1])
    later.reverse()
    return later


def norm_halves(norm):
    left, right = norm[:, :LANES], norm[:, LANES:]
    at = lanes_of(left.shape)

    def joined(a, b, c, d):
        turned = [
            pltpu.roll(v, shift, 1) if shift else v
            for v, shift in zip((left, left, right, right), (a, b, c, d), strict=True)
        ]
        low = jnp.where(at < 32, turned[0], turned[1])
        return jnp.where(at < 64, low, jnp.where(at < 96, turned[2], turned[3]))

    return joined(0, 96, 64, 32), joined(96, 64, 32, 0)


def block_kernel(
    seqs,
    n_y,
    tokens_hbm,
    next_hbm,
    w_query_hbm,
    w_key_hbm,
    w_value_hbm,
    in_gate_hbm,
    forget_gate_hbm,
    bias_hbm,
    decay_hbm,
    out_hbm,
    next_out_hbm,
    tokens_ref,
    next_ref,
    w_query_ref,
    w_key_ref,
    w_value_ref,
    gate_ref,
    bias_ref,
    decay_ref,
    out_ref,
    next_out_ref,
    sems,
    out_sems,
):
    head = lax.axis_index("tp")
    count, depth = tokens_hbm.shape
    heads = in_gate_hbm.shape[0]
    span = count // seqs
    scale = HD ** (-0.5)
    moves = [
        (in_gate_hbm, gate_ref.at[pl.ds(0, heads)]),
        (forget_gate_hbm, gate_ref.at[pl.ds(heads, heads)]),
        (tokens_hbm, tokens_ref.at[pl.ds(0, count)]),
        (bias_hbm, bias_ref),
        (decay_hbm, decay_ref),
        (w_key_hbm, w_key_ref),
        (next_hbm, next_ref),
        (w_query_hbm, w_query_ref),
        (w_value_hbm, w_value_ref),
    ]
    copies = [pltpu.make_async_copy(a, b, sems.at[i]) for i, (a, b) in enumerate(moves)]
    for copy in copies:
        copy.start()
    after = (
        lax.broadcasted_iota(jnp.int32, (span, span), 0)
        > lax.broadcasted_iota(jnp.int32, (span, span), 1)
    ).astype(BF16)
    for copy in copies:
        copy.wait()
    following = next_ref[...]
    tokens_ref[count:, :] = jnp.concatenate(
        [following.astype(F32), jnp.zeros((16 - seqs, depth), F32)], axis=0
    ).astype(BF16)

    gates = lax.dot_general(gate_ref[...], tokens_ref[...], NT, preferred_element_type=F32)
    row = lax.broadcasted_iota(jnp.int32, gates.shape, 0)
    log_in = jnp.sum(jnp.where(row == head, gates, 0.0), axis=0, keepdims=True)
    forget = jnp.sum(jnp.where(row == head + heads, gates, 0.0), axis=0, keepdims=True)
    blank = jnp.zeros((1, span - 16), F32)
    new_rows = [jnp.concatenate([v[:, count:], blank], axis=1) for v in (log_in, forget)]
    log_in, forget = (
        jnp.concatenate([v[:, p * span : (p + 1) * span] for p in range(seqs)], axis=0)
        for v in (log_in, forget)
    )
    log_forget = log_sigmoid(forget + bias_ref[head]) + decay_ref[...]
    new_rows[1] = log_sigmoid(new_rows[1] + bias_ref[head])
    split = jnp.concatenate(parts3(log_forget) + (jnp.zeros((seqs, span), F32),), axis=0)
    sums = jnp.dot(split.astype(BF16), after, preferred_element_type=F32)
    suffix = sums[:seqs] + sums[seqs : 2 * seqs] + sums[2 * seqs : 3 * seqs]
    total = jnp.sum(log_forget, axis=1, keepdims=True)
    score = suffix + log_in
    peak = jnp.max(score, axis=1, keepdims=True)
    weight = jnp.exp(score - peak) * scale
    stats = [jnp.broadcast_to(v, (seqs, span)) for v in (total, peak)]
    fill = jnp.zeros((LANES - 3 * seqs - 2, span), F32)
    turned = jnp.transpose(jnp.concatenate([weight] + stats + new_rows + [fill], axis=0))

    keys = jnp.dot(tokens_ref[...], w_key_ref[...], preferred_element_type=F32)
    weighted = []
    for p in range(seqs):
        rows = slice(p * span, (p + 1) * span)
        rounded = keys[rows].astype(BF16).astype(F32)
        weighted.append((rounded * turned[:, p : p + 1]).astype(BF16))
    query = jnp.dot(following, w_query_ref[...], preferred_element_type=F32).astype(BF16)
    new_key = keys[count : count + seqs].astype(BF16).astype(F32) * scale
    query_key = jnp.sum(query.astype(F32) * new_key, axis=1, keepdims=True)

    values = jnp.dot(tokens_ref[...], w_value_ref[...], preferred_element_type=F32).astype(BF16)
    next_out_ref[:seqs, :HD] = values[count : count + seqs].astype(F32)
    wide_at = lanes_of((seqs, LANES))
    new_in, new_forget = (turned[:seqs, 3 * seqs + i : 3 * seqs + i + 1] for i in range(2))
    next_out_ref[:seqs, HD:] = jnp.where(
        wide_at == 0, query_key, jnp.where(wide_at == 1, new_in, new_forget)
    )
    next_send = pltpu.make_async_copy(
        next_out_ref, next_out_hbm.at[pl.ds(0, 8)], out_sems.at[seqs + 1]
    )
    next_send.start()
    at = lanes_of((1, LANES))
    stats = jnp.where(at < seqs, 0.0, turned[:1])
    ones = jnp.ones((8, span), BF16)
    reads_of, norms, sends = [], [], []

    def send(start, size):
        part = pl.ds(start, size)
        sends.append(
            pltpu.make_async_copy(
                out_ref.at[:, part, :], out_hbm.at[:, part, :], out_sems.at[len(sends)]
            )
        )
        sends[-1].start()

    run = HD // 4
    for p in range(seqs):
        rows = slice(p * span, (p + 1) * span)
        memory = lax.dot_general(weighted[p], values[rows], TN, preferred_element_type=F32)
        for y in range(n_y):
            pieces = [memory[r * run + y * 8 : r * run + y * 8 + 8] for r in range(4)]
            out_ref[y, p * 32 : (p + 1) * 32, :] = jnp.concatenate(pieces, axis=0).astype(BF16)
        send(p * 32, 32)
        norms.append(jnp.dot(ones, weighted[p], preferred_element_type=F32)[:1])
        along = lax.dot_general(query, weighted[p], NT, preferred_element_type=F32)[p : p + 1]
        stats = jnp.where(at == p, jnp.sum(along, axis=1, keepdims=True), stats)
        stacked = jnp.concatenate(parts3(along) + (jnp.zeros((5, span), F32),), axis=0)
        reads = jnp.dot(stacked.astype(BF16), values[rows], preferred_element_type=F32)
        reads_of.append(jnp.sum(reads, axis=0, keepdims=True))
    stats = jnp.concatenate(parts3(stats) + (jnp.zeros((1, LANES), F32),), axis=0)
    halves = norm_halves(jnp.concatenate(norms + [jnp.zeros((8 - seqs, HD), F32)], axis=0))
    for i, half in enumerate(halves):
        wide = jnp.concatenate([stats, half[:seqs]], axis=1)
        extra = jnp.concatenate(reads_of + [wide], axis=0).astype(BF16)
        for y in range(i * n_y // 2, (i + 1) * n_y // 2):
            out_ref[y, 128:136, :] = extra
    send(128, 8)
    for copy in sends + [next_send]:
        copy.wait()


def group_kernel(seqs, n_y, n_z, in_ref, out_ref):
    extras = [in_ref[y, 128:136, :].astype(F32) for y in range(n_y)]
    rows = jnp.concatenate(
        [e[4:5, :LANES] + e[5:6, :LANES] + e[6:7, :LANES] for e in extras], axis=0
    )
    query_norm, total, peak = stats_from(rows)
    later = later_sums(total)
    scores = [later[y] + peak[y : y + 1] for y in range(n_y)]
    group_total = later[0] + total[:1]
    group_peak = functools.reduce(jnp.maximum, scores)
    coef = jnp.exp(jnp.concatenate(scores, axis=0) - group_peak)
    group_norm = jnp.sum(coef * query_norm, axis=0, keepdims=True)
    tall = jnp.transpose(jnp.concatenate([coef] * (LANES // n_y), axis=0))
    per_y = [jnp.broadcast_to(tall[:8, y : y + 1], (8, HD)) for y in range(n_y)]

    at = lanes_of((1, LANES))
    total_there = pltpu.roll(jnp.broadcast_to(group_total, (8, LANES)), 4, 1)[:1]
    peak_there = pltpu.roll(jnp.broadcast_to(group_peak, (8, LANES)), 8, 1)[:1]
    packed = jnp.where(at < 4, group_norm, jnp.where(at < 8, total_there, peak_there))
    stats = jnp.concatenate(parts3(jnp.where(at < 12, packed, 0.0)), axis=0)
    reads = jnp.zeros((seqs, HD), F32)
    norms = jnp.zeros((seqs, LANES), F32)
    for y in range(n_y):
        reads += per_y[y][:seqs] * extras[y][:seqs]
        norms += per_y[y][:seqs, :LANES] * extras[y][seqs : 2 * seqs, LANES:]
    for p in range(seqs):
        memory = jnp.zeros((32, HD), F32)
        for y in range(n_y):
            memory += per_y[y][p : p + 1] * in_ref[y, p * 32 : (p + 1) * 32, :].astype(F32)
        side = jnp.concatenate([norms[p : p + 1], jnp.zeros((2, LANES), F32)], axis=0)
        tail = jnp.concatenate(
            [reads, jnp.concatenate([stats, side], axis=1), jnp.zeros((1, HD), F32)], axis=0
        )
        for r in range(n_z // seqs):
            block = jnp.concatenate([memory[r * 8 : r * 8 + 8], tail], axis=0)
            out_ref[p * (n_z // seqs) + r] = block.astype(BF16)


def final_kernel(
    seqs, n_z, n_tp, in_ref, next_ref, w_out_ref, memory_ref, norm_ref, stab_ref, head_ref
):
    z = lax.axis_index("sp_0")
    y = lax.axis_index("sp_1")
    per_prompt = n_z // seqs
    mine = z // per_prompt
    blocks = [in_ref[i].astype(F32) for i in range(n_z)]
    rows = jnp.concatenate(
        [b[12:13, :LANES] + b[13:14, :LANES] + b[14:15, :LANES] for b in blocks], axis=0
    )
    query_norm, total, peak = stats_from(rows)
    later = later_sums(total)
    scores = [later[i] + peak[i : i + 1] for i in range(n_z)]
    stab = functools.reduce(jnp.maximum, scores, later[0] + total[:1])
    coef = jnp.exp(jnp.concatenate(scores, axis=0) - stab)
    all_norm = jnp.sum(coef * query_norm, axis=0, keepdims=True)
    filled = jnp.zeros((LANES - n_z - 2, LANES), F32)
    tall = jnp.transpose(jnp.concatenate([coef, stab, all_norm, filled], axis=0))[:8]
    stab4 = tall[:seqs, n_z : n_z + 1]
    query_norm4 = tall[:seqs, n_z + 1 : n_z + 2]
    stab_ref[...] = stab[:, :seqs]

    query_state = jnp.zeros((seqs, HD), F32)
    for i in range(n_z):
        query_state += tall[:seqs, i : i + 1] * blocks[i][8:12]
    new_value = next_ref[:seqs, :HD]
    query_key, new_in, new_forget = (next_ref[:seqs, HD + i : HD + i + 1] for i in range(3))
    carried = new_forget + stab4
    top = jnp.maximum(carried, new_in)
    keep = jnp.exp(carried - top)
    take = jnp.exp(new_in - top)
    numer = keep * query_state + take * query_key * new_value
    denom = keep * query_norm4 + take * query_key
    head_out = (numer / jnp.maximum(jnp.abs(denom), 1.0)).astype(BF16)
    partial = jnp.dot(head_out, w_out_ref[...], preferred_element_type=F32).astype(BF16)
    for i in range(n_tp):
        head_ref[i] = partial

    is_mine = lanes_of(coef.shape) == mine
    own = jnp.sum(jnp.where(is_mine, coef, 0.0), axis=1, keepdims=True)
    memory = jnp.zeros((8, HD), F32)
    norm = jnp.zeros((1, LANES), F32)
    for i in range(n_z):
        memory += own[i : i + 1] * blocks[i][:8]
        norm += own[i : i + 1] * blocks[i][12:13, LANES:]
    memory_ref[...] = memory.astype(BF16)
    first = lax.rem(z, per_prompt) * 32 + lax.rem(y, 4) * 8
    turned = pltpu.roll(jnp.broadcast_to(norm, (8, LANES)), lax.rem(LANES - first, LANES), 1)
    norm_ref[...] = turned[:1, :8]


def sum_kernel(in_ref, out_ref):
    parts = in_ref[...].astype(F32)
    out_ref[...] = jnp.sum(parts, axis=0).astype(BF16)


def per_device(
    tokens,
    next_tokens,
    w_query,
    w_key,
    w_value,
    w_in_gate,
    w_forget_gate,
    forget_bias,
    extra_decay,
    w_out,
):
    seqs, span, depth = tokens.shape
    heads = w_in_gate.shape[1]
    n_z, n_y, n_tp = (lax.axis_size(a) for a in ("sp_0", "sp_1", "tp"))
    vmem = pl.BlockSpec(memory_space=pltpu.VMEM)
    hbm = pl.BlockSpec(memory_space=pltpu.HBM)
    limit = pltpu.CompilerParams(vmem_limit_bytes=16 << 20)

    sent, following = pl.pallas_call(
        functools.partial(block_kernel, seqs, n_y),
        out_shape=(
            jax.ShapeDtypeStruct((n_y, 136, HD), BF16),
            jax.ShapeDtypeStruct((64, HD + LANES), F32),
        ),
        in_specs=[hbm] * 9,
        out_specs=(hbm, hbm),
        scratch_shapes=[
            pltpu.VMEM((seqs * span + 16, depth), BF16),
            pltpu.VMEM((seqs, depth), BF16),
            pltpu.VMEM((depth, HD), BF16),
            pltpu.VMEM((depth, HD), BF16),
            pltpu.VMEM((depth, HD), BF16),
            pltpu.VMEM((2 * heads, depth), BF16),
            pltpu.SMEM((heads,), F32),
            pltpu.VMEM((seqs, span), F32),
            pltpu.VMEM((n_y, 136, HD), BF16),
            pltpu.VMEM((8, HD + LANES), F32),
            pltpu.SemaphoreType.DMA((9,)),
            pltpu.SemaphoreType.DMA((seqs + 2,)),
        ],
    )(
        tokens.reshape(seqs * span, depth),
        next_tokens,
        w_query,
        w_key,
        w_value,
        w_in_gate.T,
        w_forget_gate.T,
        forget_bias,
        extra_decay.reshape(seqs, span),
    )
    arrived = lax.all_to_all(sent, "sp_1", 0, 0, tiled=True)
    group = pl.pallas_call(
        functools.partial(group_kernel, seqs, n_y, n_z),
        out_shape=jax.ShapeDtypeStruct((n_z, 16, HD), BF16),
        in_specs=[vmem],
        out_specs=vmem,
        compiler_params=limit,
    )(arrived)
    gathered = lax.all_to_all(group, "sp_0", 0, 0, tiled=True)
    memory, norm, stab, partial = pl.pallas_call(
        functools.partial(final_kernel, seqs, n_z, n_tp),
        out_shape=(
            jax.ShapeDtypeStruct((8, HD), BF16),
            jax.ShapeDtypeStruct((1, 8), F32),
            jax.ShapeDtypeStruct((1, seqs), F32),
            jax.ShapeDtypeStruct((n_tp, seqs, depth), BF16),
        ),
        in_specs=[vmem] * 3,
        out_specs=(vmem,) * 4,
        compiler_params=limit,
    )(gathered, following, w_out)
    parts = lax.all_to_all(partial, "tp", 0, 0, tiled=True)
    read = pl.pallas_call(
        sum_kernel,
        out_shape=jax.ShapeDtypeStruct((seqs, depth), BF16),
        in_specs=[vmem],
        out_specs=vmem,
        compiler_params=limit,
    )(parts)
    return memory[None], norm, stab.reshape(seqs, 1), read


def solution(mesh):
    torus = Mesh(mesh.devices.reshape(16, 8, mesh.shape["tp"]), ("sp_0", "sp_1", "tp"))
    placed = (
        P(None, SP, None),
        P(),
        P(None, "tp"),
        P(None, "tp"),
        P(None, "tp"),
        P(),
        P(),
        P(),
        P("tp", None, SP),
        P("tp", None),
    )
    return jax.shard_map(
        per_device,
        mesh=torus,
        in_specs=placed,
        out_specs=(P("tp", SP, None), P("tp", SP), P(None, "tp"), P()),
        check_vma=False,
    )
```

```python
import functools

import jax
import jax.numpy as jnp
from jax import lax
from jax.experimental import pallas as pl
from jax.experimental.pallas import tpu as pltpu
from jax.sharding import Mesh
from jax.sharding import PartitionSpec as P

HD = 256
SP = ("sp_0", "sp_1")
LANES = 128
F32 = jnp.float32
BF16 = jnp.bfloat16

NT = (((1,), (1,)), ((), ()))
TN = (((0,), (0,)), ((), ()))


def parts3(x):
    hi = x.astype(BF16).astype(F32)
    rest = x - hi
    mid = rest.astype(BF16).astype(F32)
    return hi, mid, rest - mid


def log_sigmoid(x):
    return jnp.minimum(x, 0.0) - jnp.log1p(jnp.exp(-jnp.abs(x)))


def lanes_of(shape):
    return lax.broadcasted_iota(jnp.int32, shape, len(shape) - 1)


def stats_from(rows):
    return rows, pltpu.roll(rows, LANES - 4, 1), pltpu.roll(rows, LANES - 8, 1)


def later_sums(total):
    later = [jnp.zeros_like(total[:1])]
    for i in range(total.shape[0] - 1, 0, -1):
        later.append(later[-1] + total[i : i + 1])
    later.reverse()
    return later


def norm_halves(norm):
    left, right = norm[:, :LANES], norm[:, LANES:]
    at = lanes_of(left.shape)

    def joined(a, b, c, d):
        turned = [
            pltpu.roll(v, shift, 1) if shift else v
            for v, shift in zip((left, left, right, right), (a, b, c, d), strict=True)
        ]
        low = jnp.where(at < 32, turned[0], turned[1])
        return jnp.where(at < 64, low, jnp.where(at < 96, turned[2], turned[3]))

    return joined(0, 96, 64, 32), joined(96, 64, 32, 0)


def block_kernel(
    seqs,
    n_y,
    tokens_hbm,
    next_hbm,
    w_query_hbm,
    w_key_hbm,
    w_value_hbm,
    in_gate_hbm,
    forget_gate_hbm,
    bias_hbm,
    decay_hbm,
    out_hbm,
    next_out_hbm,
    tokens_ref,
    next_ref,
    w_query_ref,
    w_key_ref,
    w_value_ref,
    gate_ref,
    bias_ref,
    decay_ref,
    out_ref,
    next_out_ref,
    sems,
    out_sems,
):
    head = lax.axis_index("tp")
    count, depth = tokens_hbm.shape
    heads = in_gate_hbm.shape[0]
    span = count // seqs
    scale = HD ** (-0.5)
    moves = [
        (next_hbm, next_ref),
        (in_gate_hbm, gate_ref.at[pl.ds(0, heads)]),
        (forget_gate_hbm, gate_ref.at[pl.ds(heads, heads)]),
        (tokens_hbm, tokens_ref.at[pl.ds(0, count)]),
        (bias_hbm, bias_ref),
        (decay_hbm, decay_ref),
        (w_key_hbm, w_key_ref),
        (w_query_hbm, w_query_ref),
        (w_value_hbm, w_value_ref),
    ]
    copies = [pltpu.make_async_copy(a, b, sems.at[i]) for i, (a, b) in enumerate(moves)]
    for copy in copies:
        copy.start()
    after = (
        lax.broadcasted_iota(jnp.int32, (span, span), 0)
        > lax.broadcasted_iota(jnp.int32, (span, span), 1)
    ).astype(BF16)
    for copy in copies[:6]:
        copy.wait()
    following = next_ref[...]
    tokens_ref[count:, :] = jnp.concatenate(
        [following.astype(F32), jnp.zeros((16 - seqs, depth), F32)], axis=0
    ).astype(BF16)

    gates = lax.dot_general(gate_ref[...], tokens_ref[...], NT, preferred_element_type=F32)
    row = lax.broadcasted_iota(jnp.int32, gates.shape, 0)
    log_in = jnp.sum(jnp.where(row == head, gates, 0.0), axis=0, keepdims=True)
    forget = jnp.sum(jnp.where(row == head + heads, gates, 0.0), axis=0, keepdims=True)
    blank = jnp.zeros((1, span - 16), F32)
    new_rows = [jnp.concatenate([v[:, count:], blank], axis=1) for v in (log_in, forget)]
    log_in, forget = (
        jnp.concatenate([v[:, p * span : (p + 1) * span] for p in range(seqs)], axis=0)
        for v in (log_in, forget)
    )
    log_forget = log_sigmoid(forget + bias_ref[head]) + decay_ref[...]
    new_rows[1] = log_sigmoid(new_rows[1] + bias_ref[head])
    split = jnp.concatenate(parts3(log_forget) + (jnp.zeros((seqs, span), F32),), axis=0)
    sums = jnp.dot(split.astype(BF16), after, preferred_element_type=F32)
    suffix = sums[:seqs] + sums[seqs : 2 * seqs] + sums[2 * seqs : 3 * seqs]
    total = jnp.sum(log_forget, axis=1, keepdims=True)
    score = suffix + log_in
    peak = jnp.max(score, axis=1, keepdims=True)
    weight = jnp.exp(score - peak) * scale
    stats = [jnp.broadcast_to(v, (seqs, span)) for v in (total, peak)]
    fill = jnp.zeros((LANES - 3 * seqs - 2, span), F32)
    turned = jnp.transpose(jnp.concatenate([weight] + stats + new_rows + [fill], axis=0))

    for copy in copies[6:]:
        copy.wait()
    keys = jnp.dot(tokens_ref[...], w_key_ref[...], preferred_element_type=F32)
    weighted = []
    for p in range(seqs):
        rows = slice(p * span, (p + 1) * span)
        rounded = keys[rows].astype(BF16).astype(F32)
        weighted.append((rounded * turned[:, p : p + 1]).astype(BF16))
    query = jnp.dot(following, w_query_ref[...], preferred_element_type=F32).astype(BF16)
    new_key = keys[count : count + seqs].astype(BF16).astype(F32) * scale
    query_key = jnp.sum(query.astype(F32) * new_key, axis=1, keepdims=True)

    values = jnp.dot(tokens_ref[...], w_value_ref[...], preferred_element_type=F32).astype(BF16)
    next_out_ref[:seqs, :HD] = values[count : count + seqs].astype(F32)
    wide_at = lanes_of((seqs, LANES))
    new_in, new_forget = (turned[:seqs, 3 * seqs + i : 3 * seqs + i + 1] for i in range(2))
    next_out_ref[:seqs, HD:] = jnp.where(
        wide_at == 0, query_key, jnp.where(wide_at == 1, new_in, new_forget)
    )
    next_send = pltpu.make_async_copy(
        next_out_ref, next_out_hbm.at[pl.ds(0, 8)], out_sems.at[seqs + 1]
    )
    next_send.start()
    at = lanes_of((1, LANES))
    stats = jnp.where(at < seqs, 0.0, turned[:1])
    ones = jnp.ones((8, span), BF16)
    reads_of, norms, sends = [], [], []

    def send(start, size):
        part = pl.ds(start, size)
        sends.append(
            pltpu.make_async_copy(
                out_ref.at[:, part, :], out_hbm.at[:, part, :], out_sems.at[len(sends)]
            )
        )
        sends[-1].start()

    run = HD // 4
    for p in range(seqs):
        rows = slice(p * span, (p + 1) * span)
        memory = lax.dot_general(weighted[p], values[rows], TN, preferred_element_type=F32)
        for y in range(n_y):
            pieces = [memory[r * run + y * 8 : r * run + y * 8 + 8] for r in range(4)]
            out_ref[y, p * 32 : (p + 1) * 32, :] = jnp.concatenate(pieces, axis=0).astype(BF16)
        send(p * 32, 32)
        norms.append(jnp.dot(ones, weighted[p], preferred_element_type=F32)[:1])
        along = lax.dot_general(query, weighted[p], NT, preferred_element_type=F32)[p : p + 1]
        stats = jnp.where(at == p, jnp.sum(along, axis=1, keepdims=True), stats)
        stacked = jnp.concatenate(parts3(along) + (jnp.zeros((5, span), F32),), axis=0)
        reads = jnp.dot(stacked.astype(BF16), values[rows], preferred_element_type=F32)
        reads_of.append(jnp.sum(reads, axis=0, keepdims=True))
    stats = jnp.concatenate(parts3(stats) + (jnp.zeros((1, LANES), F32),), axis=0)
    halves = norm_halves(jnp.concatenate(norms + [jnp.zeros((8 - seqs, HD), F32)], axis=0))
    for i, half in enumerate(halves):
        wide = jnp.concatenate([stats, half[:seqs]], axis=1)
        extra = jnp.concatenate(reads_of + [wide], axis=0).astype(BF16)
        for y in range(i * n_y // 2, (i + 1) * n_y // 2):
            out_ref[y, 128:136, :] = extra
    send(128, 8)
    for copy in sends + [next_send]:
        copy.wait()


def group_kernel(seqs, n_y, n_z, in_ref, out_ref):
    extras = [in_ref[y, 128:136, :].astype(F32) for y in range(n_y)]
    rows = jnp.concatenate(
        [e[4:5, :LANES] + e[5:6, :LANES] + e[6:7, :LANES] for e in extras], axis=0
    )
    query_norm, total, peak = stats_from(rows)
    later = later_sums(total)
    scores = [later[y] + peak[y : y + 1] for y in range(n_y)]
    group_total = later[0] + total[:1]
    group_peak = functools.reduce(jnp.maximum, scores)
    coef = jnp.exp(jnp.concatenate(scores, axis=0) - group_peak)
    group_norm = jnp.sum(coef * query_norm, axis=0, keepdims=True)
    tall = jnp.transpose(jnp.concatenate([coef] * (LANES // n_y), axis=0))
    per_y = [jnp.broadcast_to(tall[:8, y : y + 1], (8, HD)) for y in range(n_y)]

    at = lanes_of((1, LANES))
    total_there = pltpu.roll(jnp.broadcast_to(group_total, (8, LANES)), 4, 1)[:1]
    peak_there = pltpu.roll(jnp.broadcast_to(group_peak, (8, LANES)), 8, 1)[:1]
    packed = jnp.where(at < 4, group_norm, jnp.where(at < 8, total_there, peak_there))
    stats = jnp.concatenate(parts3(jnp.where(at < 12, packed, 0.0)), axis=0)
    reads = jnp.zeros((seqs, HD), F32)
    norms = jnp.zeros((seqs, LANES), F32)
    for y in range(n_y):
        reads += per_y[y][:seqs] * extras[y][:seqs]
        norms += per_y[y][:seqs, :LANES] * extras[y][seqs : 2 * seqs, LANES:]
    for p in range(seqs):
        memory = jnp.zeros((32, HD), F32)
        for y in range(n_y):
            memory += per_y[y][p : p + 1] * in_ref[y, p * 32 : (p + 1) * 32, :].astype(F32)
        side = jnp.concatenate([norms[p : p + 1], jnp.zeros((2, LANES), F32)], axis=0)
        tail = jnp.concatenate(
            [reads, jnp.concatenate([stats, side], axis=1), jnp.zeros((1, HD), F32)], axis=0
        )
        for r in range(n_z // seqs):
            block = jnp.concatenate([memory[r * 8 : r * 8 + 8], tail], axis=0)
            out_ref[p * (n_z // seqs) + r] = block.astype(BF16)


def final_kernel(
    seqs, n_z, n_tp, in_ref, next_ref, w_out_ref, memory_ref, rows_ref, head_ref
):
    z = lax.axis_index("sp_0")
    y = lax.axis_index("sp_1")
    per_prompt = n_z // seqs
    mine = z // per_prompt
    blocks = [in_ref[i].astype(F32) for i in range(n_z)]
    rows = jnp.concatenate(
        [b[12:13, :LANES] + b[13:14, :LANES] + b[14:15, :LANES] for b in blocks], axis=0
    )
    query_norm, total, peak = stats_from(rows)
    later = later_sums(total)
    scores = [later[i] + peak[i : i + 1] for i in range(n_z)]
    stab = functools.reduce(jnp.maximum, scores, later[0] + total[:1])
    coef = jnp.exp(jnp.concatenate(scores, axis=0) - stab)
    all_norm = jnp.sum(coef * query_norm, axis=0, keepdims=True)
    filled = jnp.zeros((LANES - n_z - 2, LANES), F32)
    tall = jnp.transpose(jnp.concatenate([coef, stab, all_norm, filled], axis=0))[:8]
    stab4 = tall[:seqs, n_z : n_z + 1]
    query_norm4 = tall[:seqs, n_z + 1 : n_z + 2]

    query_state = jnp.zeros((seqs, HD), F32)
    for i in range(n_z):
        query_state += tall[:seqs, i : i + 1] * blocks[i][8:12]
    new_value = next_ref[:seqs, :HD]
    query_key, new_in, new_forget = (next_ref[:seqs, HD + i : HD + i + 1] for i in range(3))
    carried = new_forget + stab4
    top = jnp.maximum(carried, new_in)
    keep = jnp.exp(carried - top)
    take = jnp.exp(new_in - top)
    numer = keep * query_state + take * query_key * new_value
    denom = keep * query_norm4 + take * query_key
    head_out = (numer / jnp.maximum(jnp.abs(denom), 1.0)).astype(BF16)
    partial = jnp.dot(head_out, w_out_ref[...], preferred_element_type=F32).astype(BF16)
    for i in range(n_tp):
        head_ref[i] = partial

    is_mine = lanes_of(coef.shape) == mine
    own = jnp.sum(jnp.where(is_mine, coef, 0.0), axis=1, keepdims=True)
    memory = jnp.zeros((8, HD), F32)
    norm = jnp.zeros((1, LANES), F32)
    for i in range(n_z):
        memory += own[i : i + 1] * blocks[i][:8]
        norm += own[i : i + 1] * blocks[i][12:13, LANES:]
    memory_ref[...] = memory.astype(BF16)
    first = lax.rem(z, per_prompt) * 32 + lax.rem(y, 4) * 8
    turned = pltpu.roll(jnp.broadcast_to(norm, (8, LANES)), lax.rem(LANES - first, LANES), 1)
    rows_ref[...] = jnp.concatenate([stab, turned[:7]], axis=0)


def last_kernel(seqs, in_ref, memory_in_ref, rows_ref, memory_ref, norm_ref, stab_ref, read_ref):
    memory_ref[...] = memory_in_ref[...]
    stab_ref[...] = rows_ref[:1, :seqs]
    norm_ref[...] = rows_ref[1:2, :8]
    read_ref[...] = jnp.sum(in_ref[...].astype(F32), axis=0).astype(BF16)


def per_device(
    tokens,
    next_tokens,
    w_query,
    w_key,
    w_value,
    w_in_gate,
    w_forget_gate,
    forget_bias,
    extra_decay,
    w_out,
):
    seqs, span, depth = tokens.shape
    heads = w_in_gate.shape[1]
    n_z, n_y, n_tp = (lax.axis_size(a) for a in ("sp_0", "sp_1", "tp"))
    vmem = pl.BlockSpec(memory_space=pltpu.VMEM)
    hbm = pl.BlockSpec(memory_space=pltpu.HBM)
    limit = pltpu.CompilerParams(vmem_limit_bytes=16 << 20)

    sent, following = pl.pallas_call(
        functools.partial(block_kernel, seqs, n_y),
        out_shape=(
            jax.ShapeDtypeStruct((n_y, 136, HD), BF16),
            jax.ShapeDtypeStruct((64, HD + LANES), F32),
        ),
        in_specs=[hbm] * 9,
        out_specs=(hbm, hbm),
        scratch_shapes=[
            pltpu.VMEM((seqs * span + 16, depth), BF16),
            pltpu.VMEM((seqs, depth), BF16),
            pltpu.VMEM((depth, HD), BF16),
            pltpu.VMEM((depth, HD), BF16),
            pltpu.VMEM((depth, HD), BF16),
            pltpu.VMEM((2 * heads, depth), BF16),
            pltpu.SMEM((heads,), F32),
            pltpu.VMEM((seqs, span), F32),
            pltpu.VMEM((n_y, 136, HD), BF16),
            pltpu.VMEM((8, HD + LANES), F32),
            pltpu.SemaphoreType.DMA((9,)),
            pltpu.SemaphoreType.DMA((seqs + 2,)),
        ],
    )(
        tokens.reshape(seqs * span, depth),
        next_tokens,
        w_query,
        w_key,
        w_value,
        w_in_gate.T,
        w_forget_gate.T,
        forget_bias,
        extra_decay.reshape(seqs, span),
    )
    arrived = lax.all_to_all(sent, "sp_1", 0, 0, tiled=True)
    group = pl.pallas_call(
        functools.partial(group_kernel, seqs, n_y, n_z),
        out_shape=jax.ShapeDtypeStruct((n_z, 16, HD), BF16),
        in_specs=[vmem],
        out_specs=vmem,
        compiler_params=limit,
    )(arrived)
    gathered = lax.all_to_all(group, "sp_0", 0, 0, tiled=True)
    memory_here, rows_here, partial = pl.pallas_call(
        functools.partial(final_kernel, seqs, n_z, n_tp),
        out_shape=(
            jax.ShapeDtypeStruct((8, HD), BF16),
            jax.ShapeDtypeStruct((8, LANES), F32),
            jax.ShapeDtypeStruct((n_tp, seqs, depth), BF16),
        ),
        in_specs=[vmem] * 3,
        out_specs=(vmem,) * 3,
        compiler_params=limit,
    )(gathered, following, w_out)
    parts = lax.all_to_all(partial, "tp", 0, 0, tiled=True)
    memory, norm, stab, read = pl.pallas_call(
        functools.partial(last_kernel, seqs),
        out_shape=(
            jax.ShapeDtypeStruct((8, HD), BF16),
            jax.ShapeDtypeStruct((1, 8), F32),
            jax.ShapeDtypeStruct((1, seqs), F32),
            jax.ShapeDtypeStruct((seqs, depth), BF16),
        ),
        in_specs=[vmem] * 3,
        out_specs=(vmem,) * 4,
        compiler_params=limit,
    )(parts, memory_here, rows_here)
    return memory[None], norm, stab.reshape(seqs, 1), read


def solution(mesh):
    torus = Mesh(mesh.devices.reshape(16, 8, mesh.shape["tp"]), ("sp_0", "sp_1", "tp"))
    placed = (
        P(None, SP, None),
        P(),
        P(None, "tp"),
        P(None, "tp"),
        P(None, "tp"),
        P(),
        P(),
        P(),
        P("tp", None, SP),
        P("tp", None),
    )
    return jax.shard_map(
        per_device,
        mesh=torus,
        in_specs=placed,
        out_specs=(P("tp", SP, None), P("tp", SP), P(None, "tp"), P()),
        check_vma=False,
    )
```

```python
import functools

import jax
import jax.numpy as jnp
from jax import lax
from jax.experimental import pallas as pl
from jax.experimental.pallas import tpu as pltpu
from jax.sharding import Mesh
from jax.sharding import PartitionSpec as P

HD = 256
SP = ("sp_0", "sp_1")
LANES = 128
F32 = jnp.float32
BF16 = jnp.bfloat16

NT = (((1,), (1,)), ((), ()))
TN = (((0,), (0,)), ((), ()))


def parts3(x):
    hi = x.astype(BF16).astype(F32)
    rest = x - hi
    mid = rest.astype(BF16).astype(F32)
    return hi, mid, rest - mid


def log_sigmoid(x):
    return jnp.minimum(x, 0.0) - jnp.log1p(jnp.exp(-jnp.abs(x)))


def lanes_of(shape):
    return lax.broadcasted_iota(jnp.int32, shape, len(shape) - 1)


def stats_from(rows):
    return rows, pltpu.roll(rows, LANES - 4, 1), pltpu.roll(rows, LANES - 8, 1)


def later_sums(total):
    later = [jnp.zeros_like(total[:1])]
    for i in range(total.shape[0] - 1, 0, -1):
        later.append(later[-1] + total[i : i + 1])
    later.reverse()
    return later


def norm_halves(norm):
    left, right = norm[:, :LANES], norm[:, LANES:]
    at = lanes_of(left.shape)

    def joined(a, b, c, d):
        turned = [
            pltpu.roll(v, shift, 1) if shift else v
            for v, shift in zip((left, left, right, right), (a, b, c, d), strict=True)
        ]
        low = jnp.where(at < 32, turned[0], turned[1])
        return jnp.where(at < 64, low, jnp.where(at < 96, turned[2], turned[3]))

    return joined(0, 96, 64, 32), joined(96, 64, 32, 0)


def block_kernel(
    seqs,
    n_y,
    tokens_hbm,
    next_hbm,
    w_query_hbm,
    w_key_hbm,
    w_value_hbm,
    in_gate_hbm,
    forget_gate_hbm,
    bias_hbm,
    decay_hbm,
    out_hbm,
    next_out_hbm,
    tokens_ref,
    next_ref,
    w_query_ref,
    w_key_ref,
    w_value_ref,
    gate_ref,
    bias_ref,
    decay_ref,
    out_ref,
    next_out_ref,
    sems,
    out_sems,
):
    head = lax.axis_index("tp")
    count, depth = tokens_hbm.shape
    heads = in_gate_hbm.shape[0]
    span = count // seqs
    scale = HD ** (-0.5)
    moves = [
        (next_hbm, next_ref),
        (in_gate_hbm, gate_ref.at[pl.ds(0, heads)]),
        (forget_gate_hbm, gate_ref.at[pl.ds(heads, heads)]),
        (tokens_hbm, tokens_ref.at[pl.ds(0, count)]),
        (bias_hbm, bias_ref),
        (decay_hbm, decay_ref),
        (w_key_hbm, w_key_ref),
        (w_query_hbm, w_query_ref),
        (w_value_hbm, w_value_ref),
    ]
    copies = [pltpu.make_async_copy(a, b, sems.at[i]) for i, (a, b) in enumerate(moves)]
    for copy in copies:
        copy.start()
    after = (
        lax.broadcasted_iota(jnp.int32, (span, span), 0)
        > lax.broadcasted_iota(jnp.int32, (span, span), 1)
    ).astype(BF16)
    for copy in copies[:6]:
        copy.wait()
    following = next_ref[...]
    tokens_ref[count:, :] = jnp.concatenate(
        [following.astype(F32), jnp.zeros((16 - seqs, depth), F32)], axis=0
    ).astype(BF16)

    gates = lax.dot_general(gate_ref[...], tokens_ref[...], NT, preferred_element_type=F32)
    row = lax.broadcasted_iota(jnp.int32, gates.shape, 0)
    log_in = jnp.sum(jnp.where(row == head, gates, 0.0), axis=0, keepdims=True)
    forget = jnp.sum(jnp.where(row == head + heads, gates, 0.0), axis=0, keepdims=True)
    blank = jnp.zeros((1, span - 16), F32)
    new_rows = [jnp.concatenate([v[:, count:], blank], axis=1) for v in (log_in, forget)]
    log_in, forget = (
        jnp.concatenate([v[:, p * span : (p + 1) * span] for p in range(seqs)], axis=0)
        for v in (log_in, forget)
    )
    log_forget = log_sigmoid(forget + bias_ref[head]) + decay_ref[...]
    new_rows[1] = log_sigmoid(new_rows[1] + bias_ref[head])
    split = jnp.concatenate(parts3(log_forget) + (jnp.zeros((seqs, span), F32),), axis=0)
    sums = jnp.dot(split.astype(BF16), after, preferred_element_type=F32)
    suffix = sums[:seqs] + sums[seqs : 2 * seqs] + sums[2 * seqs : 3 * seqs]
    total = jnp.sum(log_forget, axis=1, keepdims=True)
    score = suffix + log_in
    peak = jnp.max(score, axis=1, keepdims=True)
    weight = jnp.exp(score - peak) * scale
    stats = [jnp.broadcast_to(v, (seqs, span)) for v in (total, peak)]
    fill = jnp.zeros((LANES - 3 * seqs - 2, span), F32)
    turned = jnp.transpose(jnp.concatenate([weight] + stats + new_rows + [fill], axis=0))

    for copy in copies[6:]:
        copy.wait()
    keys = jnp.dot(tokens_ref[...], w_key_ref[...], preferred_element_type=F32)
    weighted = []
    for p in range(seqs):
        rows = slice(p * span, (p + 1) * span)
        rounded = keys[rows].astype(BF16).astype(F32)
        weighted.append((rounded * turned[:, p : p + 1]).astype(BF16))
    query = jnp.dot(following, w_query_ref[...], preferred_element_type=F32).astype(BF16)
    new_key = keys[count : count + seqs].astype(BF16).astype(F32) * scale
    query_key = jnp.sum(query.astype(F32) * new_key, axis=1, keepdims=True)

    values = jnp.dot(tokens_ref[...], w_value_ref[...], preferred_element_type=F32).astype(BF16)
    next_out_ref[:seqs, :HD] = values[count : count + seqs].astype(F32)
    wide_at = lanes_of((seqs, LANES))
    new_in, new_forget = (turned[:seqs, 3 * seqs + i : 3 * seqs + i + 1] for i in range(2))
    next_out_ref[:seqs, HD:] = jnp.where(
        wide_at == 0, query_key, jnp.where(wide_at == 1, new_in, new_forget)
    )
    next_send = pltpu.make_async_copy(
        next_out_ref, next_out_hbm.at[pl.ds(0, 8)], out_sems.at[seqs + 1]
    )
    next_send.start()
    at = lanes_of((1, LANES))
    stats = jnp.where(at < seqs, 0.0, turned[:1])
    ones = jnp.ones((8, span), BF16)
    reads_of, norms, sends = [], [], []

    def send(start, size):
        part = pl.ds(start, size)
        sends.append(
            pltpu.make_async_copy(
                out_ref.at[:, part, :], out_hbm.at[:, part, :], out_sems.at[len(sends)]
            )
        )
        sends[-1].start()

    run = HD // 4
    for p in range(seqs):
        rows = slice(p * span, (p + 1) * span)
        memory = lax.dot_general(weighted[p], values[rows], TN, preferred_element_type=F32)
        for y in range(n_y):
            pieces = [memory[r * run + y * 8 : r * run + y * 8 + 8] for r in range(4)]
            out_ref[y, p * 32 : (p + 1) * 32, :] = jnp.concatenate(pieces, axis=0).astype(BF16)
        send(p * 32, 32)
        norms.append(jnp.dot(ones, weighted[p], preferred_element_type=F32)[:1])
        along = lax.dot_general(query, weighted[p], NT, preferred_element_type=F32)[p : p + 1]
        stats = jnp.where(at == p, jnp.sum(along, axis=1, keepdims=True), stats)
        stacked = jnp.concatenate(parts3(along) + (jnp.zeros((5, span), F32),), axis=0)
        reads = jnp.dot(stacked.astype(BF16), values[rows], preferred_element_type=F32)
        reads_of.append(jnp.sum(reads, axis=0, keepdims=True))
    stats = jnp.concatenate(parts3(stats) + (jnp.zeros((1, LANES), F32),), axis=0)
    halves = norm_halves(jnp.concatenate(norms + [jnp.zeros((8 - seqs, HD), F32)], axis=0))
    for i, half in enumerate(halves):
        wide = jnp.concatenate([stats, half[:seqs]], axis=1)
        extra = jnp.concatenate(reads_of + [wide], axis=0).astype(BF16)
        for y in range(i * n_y // 2, (i + 1) * n_y // 2):
            out_ref[y, 128:136, :] = extra
    send(128, 8)
    for copy in sends + [next_send]:
        copy.wait()


def group_kernel(seqs, n_y, n_z, in_ref, out_ref):
    extras = [in_ref[y, 128:136, :].astype(F32) for y in range(n_y)]
    rows = jnp.concatenate(
        [e[4:5, :LANES] + e[5:6, :LANES] + e[6:7, :LANES] for e in extras], axis=0
    )
    query_norm, total, peak = stats_from(rows)
    later = later_sums(total)
    scores = [later[y] + peak[y : y + 1] for y in range(n_y)]
    group_total = later[0] + total[:1]
    group_peak = functools.reduce(jnp.maximum, scores)
    coef = jnp.exp(jnp.concatenate(scores, axis=0) - group_peak)
    group_norm = jnp.sum(coef * query_norm, axis=0, keepdims=True)
    tall = jnp.transpose(jnp.concatenate([coef] * (LANES // n_y), axis=0))
    per_y = [jnp.broadcast_to(tall[:8, y : y + 1], (8, HD)) for y in range(n_y)]

    at = lanes_of((1, LANES))
    total_there = pltpu.roll(jnp.broadcast_to(group_total, (8, LANES)), 4, 1)[:1]
    peak_there = pltpu.roll(jnp.broadcast_to(group_peak, (8, LANES)), 8, 1)[:1]
    packed = jnp.where(at < 4, group_norm, jnp.where(at < 8, total_there, peak_there))
    stats = jnp.concatenate(parts3(jnp.where(at < 12, packed, 0.0)), axis=0)
    reads = jnp.zeros((seqs, HD), F32)
    norms = jnp.zeros((seqs, LANES), F32)
    for y in range(n_y):
        reads += per_y[y][:seqs] * extras[y][:seqs]
        norms += per_y[y][:seqs, :LANES] * extras[y][seqs : 2 * seqs, LANES:]
    for p in range(seqs):
        memory = jnp.zeros((32, HD), F32)
        for y in range(n_y):
            memory += per_y[y][p : p + 1] * in_ref[y, p * 32 : (p + 1) * 32, :].astype(F32)
        side = jnp.concatenate([norms[p : p + 1], jnp.zeros((2, LANES), F32)], axis=0)
        tail = jnp.concatenate(
            [reads, jnp.concatenate([stats, side], axis=1), jnp.zeros((1, HD), F32)], axis=0
        )
        for r in range(n_z // seqs):
            block = jnp.concatenate([memory[r * 8 : r * 8 + 8], tail], axis=0)
            out_ref[n_z - 1 - p * (n_z // seqs) - r] = block.astype(BF16)


def final_kernel(
    seqs, n_z, n_tp, in_ref, next_ref, w_out_ref, memory_ref, rows_ref, head_ref
):
    z = lax.axis_index("sp_0")
    y = lax.axis_index("sp_1")
    per_prompt = n_z // seqs
    mine = z // per_prompt
    blocks = [in_ref[n_z - 1 - i].astype(F32) for i in range(n_z)]
    rows = jnp.concatenate(
        [b[12:13, :LANES] + b[13:14, :LANES] + b[14:15, :LANES] for b in blocks], axis=0
    )
    query_norm, total, peak = stats_from(rows)
    later = later_sums(total)
    scores = [later[i] + peak[i : i + 1] for i in range(n_z)]
    stab = functools.reduce(jnp.maximum, scores, later[0] + total[:1])
    coef = jnp.exp(jnp.concatenate(scores, axis=0) - stab)
    all_norm = jnp.sum(coef * query_norm, axis=0, keepdims=True)
    filled = jnp.zeros((LANES - n_z - 2, LANES), F32)
    tall = jnp.transpose(jnp.concatenate([coef, stab, all_norm, filled], axis=0))[:8]
    stab4 = tall[:seqs, n_z : n_z + 1]
    query_norm4 = tall[:seqs, n_z + 1 : n_z + 2]

    query_state = jnp.zeros((seqs, HD), F32)
    for i in range(n_z):
        query_state += tall[:seqs, i : i + 1] * blocks[i][8:12]
    new_value = next_ref[:seqs, :HD]
    query_key, new_in, new_forget = (next_ref[:seqs, HD + i : HD + i + 1] for i in range(3))
    carried = new_forget + stab4
    top = jnp.maximum(carried, new_in)
    keep = jnp.exp(carried - top)
    take = jnp.exp(new_in - top)
    numer = keep * query_state + take * query_key * new_value
    denom = keep * query_norm4 + take * query_key
    head_out = (numer / jnp.maximum(jnp.abs(denom), 1.0)).astype(BF16)
    partial = jnp.dot(head_out, w_out_ref[...], preferred_element_type=F32).astype(BF16)
    for i in range(n_tp):
        head_ref[i] = partial

    is_mine = lanes_of(coef.shape) == mine
    own = jnp.sum(jnp.where(is_mine, coef, 0.0), axis=1, keepdims=True)
    memory = jnp.zeros((8, HD), F32)
    norm = jnp.zeros((1, LANES), F32)
    for i in range(n_z):
        memory += own[i : i + 1] * blocks[i][:8]
        norm += own[i : i + 1] * blocks[i][12:13, LANES:]
    memory_ref[...] = memory.astype(BF16)
    first = lax.rem(z, per_prompt) * 32 + lax.rem(y, 4) * 8
    turned = pltpu.roll(jnp.broadcast_to(norm, (8, LANES)), lax.rem(LANES - first, LANES), 1)
    rows_ref[...] = jnp.concatenate([stab, turned[:7]], axis=0)


def last_kernel(seqs, in_ref, memory_in_ref, rows_ref, memory_ref, norm_ref, stab_ref, read_ref):
    memory_ref[...] = memory_in_ref[...]
    stab_ref[...] = rows_ref[:1, :seqs]
    norm_ref[...] = rows_ref[1:2, :8]
    read_ref[...] = jnp.sum(in_ref[...].astype(F32), axis=0).astype(BF16)


def exchange_backwards(blocks, axis):
    backwards = list(range(lax.axis_size(axis)))[::-1]
    return lax.all_to_all(blocks, axis, 0, 0, tiled=True, axis_index_groups=[backwards])


def per_device(
    tokens,
    next_tokens,
    w_query,
    w_key,
    w_value,
    w_in_gate,
    w_forget_gate,
    forget_bias,
    extra_decay,
    w_out,
):
    seqs, span, depth = tokens.shape
    heads = w_in_gate.shape[1]
    n_z, n_y, n_tp = (lax.axis_size(a) for a in ("sp_0", "sp_1", "tp"))
    vmem = pl.BlockSpec(memory_space=pltpu.VMEM)
    hbm = pl.BlockSpec(memory_space=pltpu.HBM)
    limit = pltpu.CompilerParams(vmem_limit_bytes=16 << 20)

    sent, following = pl.pallas_call(
        functools.partial(block_kernel, seqs, n_y),
        out_shape=(
            jax.ShapeDtypeStruct((n_y, 136, HD), BF16),
            jax.ShapeDtypeStruct((64, HD + LANES), F32),
        ),
        in_specs=[hbm] * 9,
        out_specs=(hbm, hbm),
        scratch_shapes=[
            pltpu.VMEM((seqs * span + 16, depth), BF16),
            pltpu.VMEM((seqs, depth), BF16),
            pltpu.VMEM((depth, HD), BF16),
            pltpu.VMEM((depth, HD), BF16),
            pltpu.VMEM((depth, HD), BF16),
            pltpu.VMEM((2 * heads, depth), BF16),
            pltpu.SMEM((heads,), F32),
            pltpu.VMEM((seqs, span), F32),
            pltpu.VMEM((n_y, 136, HD), BF16),
            pltpu.VMEM((8, HD + LANES), F32),
            pltpu.SemaphoreType.DMA((9,)),
            pltpu.SemaphoreType.DMA((seqs + 2,)),
        ],
    )(
        tokens.reshape(seqs * span, depth),
        next_tokens,
        w_query,
        w_key,
        w_value,
        w_in_gate.T,
        w_forget_gate.T,
        forget_bias,
        extra_decay.reshape(seqs, span),
    )
    arrived = lax.all_to_all(sent, "sp_1", 0, 0, tiled=True)
    group = pl.pallas_call(
        functools.partial(group_kernel, seqs, n_y, n_z),
        out_shape=jax.ShapeDtypeStruct((n_z, 16, HD), BF16),
        in_specs=[vmem],
        out_specs=vmem,
        compiler_params=limit,
    )(arrived)
    gathered = exchange_backwards(group, "sp_0")
    memory_here, rows_here, partial = pl.pallas_call(
        functools.partial(final_kernel, seqs, n_z, n_tp),
        out_shape=(
            jax.ShapeDtypeStruct((8, HD), BF16),
            jax.ShapeDtypeStruct((8, LANES), F32),
            jax.ShapeDtypeStruct((n_tp, seqs, depth), BF16),
        ),
        in_specs=[vmem] * 3,
        out_specs=(vmem,) * 3,
        compiler_params=limit,
    )(gathered, following, w_out)
    parts = exchange_backwards(partial, "tp")
    memory, norm, stab, read = pl.pallas_call(
        functools.partial(last_kernel, seqs),
        out_shape=(
            jax.ShapeDtypeStruct((8, HD), BF16),
            jax.ShapeDtypeStruct((1, 8), F32),
            jax.ShapeDtypeStruct((1, seqs), F32),
            jax.ShapeDtypeStruct((seqs, depth), BF16),
        ),
        in_specs=[vmem] * 3,
        out_specs=(vmem,) * 4,
        compiler_params=limit,
    )(parts, memory_here, rows_here)
    return memory[None], norm, stab.reshape(seqs, 1), read


def solution(mesh):
    torus = Mesh(mesh.devices.reshape(16, 8, mesh.shape["tp"]), ("sp_0", "sp_1", "tp"))
    placed = (
        P(None, SP, None),
        P(),
        P(None, "tp"),
        P(None, "tp"),
        P(None, "tp"),
        P(),
        P(),
        P(),
        P("tp", None, SP),
        P("tp", None),
    )
    return jax.shard_map(
        per_device,
        mesh=torus,
        in_specs=placed,
        out_specs=(P("tp", SP, None), P("tp", SP), P(None, "tp"), P()),
        check_vma=False,
    )
```

```python
import functools

import jax
import jax.numpy as jnp
from jax import lax
from jax.experimental import pallas as pl
from jax.experimental.pallas import tpu as pltpu
from jax.sharding import Mesh
from jax.sharding import PartitionSpec as P

HD = 256
SP = ("sp_0", "sp_1")
LANES = 128
F32 = jnp.float32
BF16 = jnp.bfloat16

NT = (((1,), (1,)), ((), ()))
TN = (((0,), (0,)), ((), ()))


def parts3(x):
    hi = x.astype(BF16).astype(F32)
    rest = x - hi
    mid = rest.astype(BF16).astype(F32)
    return hi, mid, rest - mid


def log_sigmoid(x):
    return jnp.minimum(x, 0.0) - jnp.log1p(jnp.exp(-jnp.abs(x)))


def lanes_of(shape):
    return lax.broadcasted_iota(jnp.int32, shape, len(shape) - 1)


def stats_from(rows):
    return rows, pltpu.roll(rows, LANES - 4, 1), pltpu.roll(rows, LANES - 8, 1)


def later_sums(total):
    later = [jnp.zeros_like(total[:1])]
    for i in range(total.shape[0] - 1, 0, -1):
        later.append(later[-1] + total[i : i + 1])
    later.reverse()
    return later


def norm_halves(norm):
    left, right = norm[:, :LANES], norm[:, LANES:]
    at = lanes_of(left.shape)

    def joined(a, b, c, d):
        turned = [
            pltpu.roll(v, shift, 1) if shift else v
            for v, shift in zip((left, left, right, right), (a, b, c, d), strict=True)
        ]
        low = jnp.where(at < 32, turned[0], turned[1])
        return jnp.where(at < 64, low, jnp.where(at < 96, turned[2], turned[3]))

    return joined(0, 96, 64, 32), joined(96, 64, 32, 0)


def block_kernel(
    seqs,
    n_y,
    tokens_hbm,
    next_hbm,
    w_query_hbm,
    w_key_hbm,
    w_value_hbm,
    in_gate_hbm,
    forget_gate_hbm,
    bias_hbm,
    decay_hbm,
    out_hbm,
    next_out_hbm,
    tokens_ref,
    next_ref,
    w_query_ref,
    w_key_ref,
    w_value_ref,
    gate_ref,
    bias_ref,
    decay_ref,
    out_ref,
    next_out_ref,
    sems,
    out_sems,
):
    head = lax.axis_index("tp")
    count, depth = tokens_hbm.shape
    heads = in_gate_hbm.shape[0]
    span = count // seqs
    scale = HD ** (-0.5)
    moves = [
        (next_hbm, next_ref),
        (in_gate_hbm, gate_ref.at[pl.ds(0, heads)]),
        (forget_gate_hbm, gate_ref.at[pl.ds(heads, heads)]),
        (tokens_hbm, tokens_ref.at[pl.ds(0, count)]),
        (bias_hbm, bias_ref),
        (decay_hbm, decay_ref),
        (w_key_hbm, w_key_ref),
        (w_query_hbm, w_query_ref),
        (w_value_hbm, w_value_ref),
    ]
    copies = [pltpu.make_async_copy(a, b, sems.at[i]) for i, (a, b) in enumerate(moves)]
    for copy in copies:
        copy.start()
    after = (
        lax.broadcasted_iota(jnp.int32, (span, span), 0)
        > lax.broadcasted_iota(jnp.int32, (span, span), 1)
    ).astype(BF16)
    for copy in copies[:6]:
        copy.wait()
    following = next_ref[...]
    tokens_ref[count:, :] = jnp.concatenate(
        [following.astype(F32), jnp.zeros((16 - seqs, depth), F32)], axis=0
    ).astype(BF16)

    gates = lax.dot_general(gate_ref[...], tokens_ref[...], NT, preferred_element_type=F32)
    row = lax.broadcasted_iota(jnp.int32, gates.shape, 0)
    log_in = jnp.sum(jnp.where(row == head, gates, 0.0), axis=0, keepdims=True)
    forget = jnp.sum(jnp.where(row == head + heads, gates, 0.0), axis=0, keepdims=True)
    blank = jnp.zeros((1, span - 16), F32)
    new_rows = [jnp.concatenate([v[:, count:], blank], axis=1) for v in (log_in, forget)]
    log_in, forget = (
        jnp.concatenate([v[:, p * span : (p + 1) * span] for p in range(seqs)], axis=0)
        for v in (log_in, forget)
    )
    log_forget = log_sigmoid(forget + bias_ref[head]) + decay_ref[...]
    new_rows[1] = log_sigmoid(new_rows[1] + bias_ref[head])
    split = jnp.concatenate(parts3(log_forget) + (jnp.zeros((seqs, span), F32),), axis=0)
    sums = jnp.dot(split.astype(BF16), after, preferred_element_type=F32)
    suffix = sums[:seqs] + sums[seqs : 2 * seqs] + sums[2 * seqs : 3 * seqs]
    total = jnp.sum(log_forget, axis=1, keepdims=True)
    score = suffix + log_in
    peak = jnp.max(score, axis=1, keepdims=True)
    weight = jnp.exp(score - peak) * scale
    stats = [jnp.broadcast_to(v, (seqs, span)) for v in (total, peak)]
    fill = jnp.zeros((LANES - 3 * seqs - 2, span), F32)
    turned = jnp.transpose(jnp.concatenate([weight] + stats + new_rows + [fill], axis=0))

    for copy in copies[6:]:
        copy.wait()
    keys = jnp.dot(tokens_ref[...], w_key_ref[...], preferred_element_type=F32)
    weighted = []
    for p in range(seqs):
        rows = slice(p * span, (p + 1) * span)
        rounded = keys[rows].astype(BF16).astype(F32)
        weighted.append((rounded * turned[:, p : p + 1]).astype(BF16))
    query = jnp.dot(following, w_query_ref[...], preferred_element_type=F32).astype(BF16)
    new_key = keys[count : count + seqs].astype(BF16).astype(F32) * scale
    query_key = jnp.sum(query.astype(F32) * new_key, axis=1, keepdims=True)

    values = jnp.dot(tokens_ref[...], w_value_ref[...], preferred_element_type=F32).astype(BF16)
    next_out_ref[:seqs, :HD] = values[count : count + seqs].astype(F32)
    wide_at = lanes_of((seqs, LANES))
    new_in, new_forget = (turned[:seqs, 3 * seqs + i : 3 * seqs + i + 1] for i in range(2))
    next_out_ref[:seqs, HD:] = jnp.where(
        wide_at == 0, query_key, jnp.where(wide_at == 1, new_in, new_forget)
    )
    next_send = pltpu.make_async_copy(
        next_out_ref, next_out_hbm.at[pl.ds(0, 8)], out_sems.at[seqs + 1]
    )
    next_send.start()
    at = lanes_of((1, LANES))
    stats = jnp.where(at < seqs, 0.0, turned[:1])
    ones = jnp.ones((8, span), BF16)
    reads_of, norms, sends = [], [], []

    def send(start, size):
        part = pl.ds(start, size)
        sends.append(
            pltpu.make_async_copy(
                out_ref.at[:, part, :], out_hbm.at[:, part, :], out_sems.at[len(sends)]
            )
        )
        sends[-1].start()

    run = HD // 4
    for p in range(seqs):
        rows = slice(p * span, (p + 1) * span)
        memory = lax.dot_general(weighted[p], values[rows], TN, preferred_element_type=F32)
        for y in range(n_y):
            pieces = [memory[r * run + y * 8 : r * run + y * 8 + 8] for r in range(4)]
            out_ref[y, p * 32 : (p + 1) * 32, :] = jnp.concatenate(pieces, axis=0).astype(BF16)
        send(p * 32, 32)
        norms.append(jnp.dot(ones, weighted[p], preferred_element_type=F32)[:1])
        along = lax.dot_general(query, weighted[p], NT, preferred_element_type=F32)[p : p + 1]
        stats = jnp.where(at == p, jnp.sum(along, axis=1, keepdims=True), stats)
        stacked = jnp.concatenate(parts3(along) + (jnp.zeros((5, span), F32),), axis=0)
        reads = jnp.dot(stacked.astype(BF16), values[rows], preferred_element_type=F32)
        reads_of.append(jnp.sum(reads, axis=0, keepdims=True))
    stats = jnp.concatenate(parts3(stats) + (jnp.zeros((1, LANES), F32),), axis=0)
    halves = norm_halves(jnp.concatenate(norms + [jnp.zeros((8 - seqs, HD), F32)], axis=0))
    for i, half in enumerate(halves):
        wide = jnp.concatenate([stats, half[:seqs]], axis=1)
        extra = jnp.concatenate(reads_of + [wide], axis=0).astype(BF16)
        for y in range(i * n_y // 2, (i + 1) * n_y // 2):
            out_ref[y, 128:136, :] = extra
    send(128, 8)
    for copy in sends + [next_send]:
        copy.wait()


def group_kernel(seqs, n_y, n_z, in_ref, out_ref):
    extras = [in_ref[y, 128:136, :].astype(F32) for y in range(n_y)]
    rows = jnp.concatenate(
        [e[4:5, :LANES] + e[5:6, :LANES] + e[6:7, :LANES] for e in extras], axis=0
    )
    query_norm, total, peak = stats_from(rows)
    later = later_sums(total)
    scores = [later[y] + peak[y : y + 1] for y in range(n_y)]
    group_total = later[0] + total[:1]
    group_peak = functools.reduce(jnp.maximum, scores)
    coef = jnp.exp(jnp.concatenate(scores, axis=0) - group_peak)
    group_norm = jnp.sum(coef * query_norm, axis=0, keepdims=True)
    tall = jnp.transpose(jnp.concatenate([coef] * (LANES // n_y), axis=0))
    per_y = [jnp.broadcast_to(tall[:8, y : y + 1], (8, HD)) for y in range(n_y)]

    at = lanes_of((1, LANES))
    total_there = pltpu.roll(jnp.broadcast_to(group_total, (8, LANES)), 4, 1)[:1]
    peak_there = pltpu.roll(jnp.broadcast_to(group_peak, (8, LANES)), 8, 1)[:1]
    packed = jnp.where(at < 4, group_norm, jnp.where(at < 8, total_there, peak_there))
    stats = jnp.concatenate(parts3(jnp.where(at < 12, packed, 0.0)), axis=0)
    reads = jnp.zeros((seqs, HD), F32)
    norms = jnp.zeros((seqs, LANES), F32)
    for y in range(n_y):
        reads += per_y[y][:seqs] * extras[y][:seqs]
        norms += per_y[y][:seqs, :LANES] * extras[y][seqs : 2 * seqs, LANES:]
    for p in range(seqs):
        memory = jnp.zeros((32, HD), F32)
        for y in range(n_y):
            memory += per_y[y][p : p + 1] * in_ref[y, p * 32 : (p + 1) * 32, :].astype(F32)
        side = jnp.concatenate([norms[p : p + 1], jnp.zeros((2, LANES), F32)], axis=0)
        tail = jnp.concatenate(
            [reads, jnp.concatenate([stats, side], axis=1), jnp.zeros((1, HD), F32)], axis=0
        )
        for r in range(n_z // seqs):
            block = jnp.concatenate([memory[r * 8 : r * 8 + 8], tail], axis=0)
            out_ref[9 * (p * (n_z // seqs) + r) % n_z] = block.astype(BF16)


def final_kernel(
    seqs, n_z, n_tp, in_ref, next_ref, w_out_ref, memory_ref, rows_ref, head_ref
):
    z = lax.axis_index("sp_0")
    y = lax.axis_index("sp_1")
    per_prompt = n_z // seqs
    mine = z // per_prompt
    blocks = [in_ref[9 * i % n_z].astype(F32) for i in range(n_z)]
    rows = jnp.concatenate(
        [b[12:13, :LANES] + b[13:14, :LANES] + b[14:15, :LANES] for b in blocks], axis=0
    )
    query_norm, total, peak = stats_from(rows)
    later = later_sums(total)
    scores = [later[i] + peak[i : i + 1] for i in range(n_z)]
    stab = functools.reduce(jnp.maximum, scores, later[0] + total[:1])
    coef = jnp.exp(jnp.concatenate(scores, axis=0) - stab)
    all_norm = jnp.sum(coef * query_norm, axis=0, keepdims=True)
    filled = jnp.zeros((LANES - n_z - 2, LANES), F32)
    tall = jnp.transpose(jnp.concatenate([coef, stab, all_norm, filled], axis=0))[:8]
    stab4 = tall[:seqs, n_z : n_z + 1]
    query_norm4 = tall[:seqs, n_z + 1 : n_z + 2]

    query_state = jnp.zeros((seqs, HD), F32)
    for i in range(n_z):
        query_state += tall[:seqs, i : i + 1] * blocks[i][8:12]
    new_value = next_ref[:seqs, :HD]
    query_key, new_in, new_forget = (next_ref[:seqs, HD + i : HD + i + 1] for i in range(3))
    carried = new_forget + stab4
    top = jnp.maximum(carried, new_in)
    keep = jnp.exp(carried - top)
    take = jnp.exp(new_in - top)
    numer = keep * query_state + take * query_key * new_value
    denom = keep * query_norm4 + take * query_key
    head_out = (numer / jnp.maximum(jnp.abs(denom), 1.0)).astype(BF16)
    partial = jnp.dot(head_out, w_out_ref[...], preferred_element_type=F32).astype(BF16)
    for i in range(n_tp):
        head_ref[i] = partial

    is_mine = lanes_of(coef.shape) == mine
    own = jnp.sum(jnp.where(is_mine, coef, 0.0), axis=1, keepdims=True)
    memory = jnp.zeros((8, HD), F32)
    norm = jnp.zeros((1, LANES), F32)
    for i in range(n_z):
        memory += own[i : i + 1] * blocks[i][:8]
        norm += own[i : i + 1] * blocks[i][12:13, LANES:]
    memory_ref[...] = memory.astype(BF16)
    first = lax.rem(z, per_prompt) * 32 + lax.rem(y, 4) * 8
    turned = pltpu.roll(jnp.broadcast_to(norm, (8, LANES)), lax.rem(LANES - first, LANES), 1)
    rows_ref[...] = jnp.concatenate([stab, turned[:7]], axis=0)


def last_kernel(seqs, in_ref, memory_in_ref, rows_ref, memory_ref, norm_ref, stab_ref, read_ref):
    memory_ref[...] = memory_in_ref[...]
    stab_ref[...] = rows_ref[:1, :seqs]
    norm_ref[...] = rows_ref[1:2, :8]
    read_ref[...] = jnp.sum(in_ref[...].astype(F32), axis=0).astype(BF16)


def exchange_backwards(blocks, axis):
    backwards = list(range(lax.axis_size(axis)))[::-1]
    return lax.all_to_all(blocks, axis, 0, 0, tiled=True, axis_index_groups=[backwards])


def per_device(
    tokens,
    next_tokens,
    w_query,
    w_key,
    w_value,
    w_in_gate,
    w_forget_gate,
    forget_bias,
    extra_decay,
    w_out,
):
    seqs, span, depth = tokens.shape
    heads = w_in_gate.shape[1]
    n_z, n_y, n_tp = (lax.axis_size(a) for a in ("sp_0", "sp_1", "tp"))
    vmem = pl.BlockSpec(memory_space=pltpu.VMEM)
    hbm = pl.BlockSpec(memory_space=pltpu.HBM)
    limit = pltpu.CompilerParams(vmem_limit_bytes=16 << 20)

    sent, following = pl.pallas_call(
        functools.partial(block_kernel, seqs, n_y),
        out_shape=(
            jax.ShapeDtypeStruct((n_y, 136, HD), BF16),
            jax.ShapeDtypeStruct((64, HD + LANES), F32),
        ),
        in_specs=[hbm] * 9,
        out_specs=(hbm, hbm),
        scratch_shapes=[
            pltpu.VMEM((seqs * span + 16, depth), BF16),
            pltpu.VMEM((seqs, depth), BF16),
            pltpu.VMEM((depth, HD), BF16),
            pltpu.VMEM((depth, HD), BF16),
            pltpu.VMEM((depth, HD), BF16),
            pltpu.VMEM((2 * heads, depth), BF16),
            pltpu.SMEM((heads,), F32),
            pltpu.VMEM((seqs, span), F32),
            pltpu.VMEM((n_y, 136, HD), BF16),
            pltpu.VMEM((8, HD + LANES), F32),
            pltpu.SemaphoreType.DMA((9,)),
            pltpu.SemaphoreType.DMA((seqs + 2,)),
        ],
    )(
        tokens.reshape(seqs * span, depth),
        next_tokens,
        w_query,
        w_key,
        w_value,
        w_in_gate.T,
        w_forget_gate.T,
        forget_bias,
        extra_decay.reshape(seqs, span),
    )
    arrived = lax.all_to_all(sent, "sp_1", 0, 0, tiled=True)
    group = pl.pallas_call(
        functools.partial(group_kernel, seqs, n_y, n_z),
        out_shape=jax.ShapeDtypeStruct((n_z, 16, HD), BF16),
        in_specs=[vmem],
        out_specs=vmem,
        compiler_params=limit,
    )(arrived)
    steps = [[9 * i % n_z for i in range(n_z)]]
    gathered = lax.all_to_all(group, "sp_0", 0, 0, tiled=True, axis_index_groups=steps)
    memory_here, rows_here, partial = pl.pallas_call(
        functools.partial(final_kernel, seqs, n_z, n_tp),
        out_shape=(
            jax.ShapeDtypeStruct((8, HD), BF16),
            jax.ShapeDtypeStruct((8, LANES), F32),
            jax.ShapeDtypeStruct((n_tp, seqs, depth), BF16),
        ),
        in_specs=[vmem] * 3,
        out_specs=(vmem,) * 3,
        compiler_params=limit,
    )(gathered, following, w_out)
    parts = exchange_backwards(partial, "tp")
    memory, norm, stab, read = pl.pallas_call(
        functools.partial(last_kernel, seqs),
        out_shape=(
            jax.ShapeDtypeStruct((8, HD), BF16),
            jax.ShapeDtypeStruct((1, 8), F32),
            jax.ShapeDtypeStruct((1, seqs), F32),
            jax.ShapeDtypeStruct((seqs, depth), BF16),
        ),
        in_specs=[vmem] * 3,
        out_specs=(vmem,) * 4,
        compiler_params=limit,
    )(parts, memory_here, rows_here)
    return memory[None], norm, stab.reshape(seqs, 1), read


def solution(mesh):
    torus = Mesh(mesh.devices.reshape(16, 8, mesh.shape["tp"]), ("sp_0", "sp_1", "tp"))
    placed = (
        P(None, SP, None),
        P(),
        P(None, "tp"),
        P(None, "tp"),
        P(None, "tp"),
        P(),
        P(),
        P(),
        P("tp", None, SP),
        P("tp", None),
    )
    return jax.shard_map(
        per_device,
        mesh=torus,
        in_specs=placed,
        out_specs=(P("tp", SP, None), P("tp", SP), P(None, "tp"), P()),
        check_vma=False,
    )
```
